512 devices in a mesh: grp: 2 (over y), fs: 64 (over z, core), tp: 4 (over x).
Axes of the slice: x: 4, y: 2, z: 32, core: 2. Of those that a mesh axis runs over, the one named last changes fastest.
The devices are a block of a 4x8x32 slice.
Arguments:
- tokens: bfloat16 [2048, 3072], P(('grp', 'tp')), parts along dimension 0, may hold values from -6 to 6
- up_master: float32 [3072, 12288], P('fs', 'tp'), may hold values from -0.109375 to 0.109375
- down_master: float32 [12288, 3072], P('fs', 'tp'), may hold values from -0.0546875 to 0.0546875
- norm_gain: float32 [3072], P('fs'), may hold values from 0.1 to 1.9
Outputs:
- prompt_out: bfloat16 [2048, 3072], P(('grp', 'tp'), 'fs'), parts along dimension 0
- sampled_up: bfloat16 [6144, 12288], P('grp', 'fs'), parts along dimension 0
- sampled_down: bfloat16 [24576, 3072], P(('grp', 'fs')), parts along dimension 0
The draws below stay inside these ranges and needn't reach their ends.
There are 2 independent parts, one for each index of `grp`. The reference program is written for one: setup_inputs(seed, part) draws one part's arguments, and reference() takes and returns one part's arrays. A program takes and returns all parts, laid end to end along the dimension named above; an argument that names none is the same for every part. Nothing has to cross between parts.
All inputs are finite; a program needn't handle non-finite values.
Results may differ from the reference program's by a relative error of at most 0.0074.
Values may be sent and summed in bfloat16 or wider, within the bound.
A program may use at most 64 MiB of HBM per device.

```python
import jax
import jax.numpy as jnp
from jax import lax

D = 3072
FF = 12288
TOKENS = 1024


def block_levels(own_key, shape, split, low, high):
    level = 1.0
    for position, parts in split:
        steps = jax.random.uniform(jax.random.fold_in(jax.random.fold_in(own_key, 6), position), (parts,), jnp.float32, low / len(split), high / len(split))
        level = level * jnp.repeat(jnp.exp(steps), shape[position] // parts).reshape((-1,) + (1,) * (len(shape) - 1 - position))
    return level


def normal_values(key, shape, scale, limit, split=(), held_as=jnp.bfloat16):
    factor_of = block_levels(key, shape, split, -0.22, 0.18) if split else 1.0
    array = jax.random.normal(key, shape, jnp.float32) * scale * factor_of
    return jnp.minimum(jnp.maximum(array, -limit), limit).astype(held_as)


def setup_inputs(seed: int = 0, part: int = 0) -> dict:
    keys = jax.random.split(jax.random.key(seed), 5)
    own_keys = jax.random.split(jax.random.fold_in(keys[4], part), 5)
    return {
        "tokens": normal_values(own_keys[0], (TOKENS, D), 1.0, 6.0, ((0, 4),)),
        "up_master": normal_values(keys[1], (D, FF), D ** -0.5, 0.109375, ((0, 64), (1, 4)), jnp.float32),
        "down_master": normal_values(keys[2], (FF, D), FF ** -0.5, 0.0546875, ((0, 64), (1, 4)), jnp.float32),
        "norm_gain": jnp.clip(1.0 + 0.18 * jax.random.normal(keys[3], (D,), jnp.float32), 0.1, 1.9),
    }


def reference(tokens, up_master, down_master, norm_gain):
    sampled_up = (norm_gain[:, None] * up_master).astype(jnp.bfloat16)
    sampled_down = down_master.astype(jnp.bfloat16)
    values = tokens.astype(jnp.float32)
    center = lax.optimization_barrier(jnp.mean(values, axis=-1, keepdims=True))
    spread = lax.optimization_barrier(jnp.mean(jnp.square(values - center), axis=-1, keepdims=True))
    normalized = ((values - center) * lax.rsqrt(spread + 1e-05)).astype(jnp.bfloat16)
    before = jnp.dot(normalized, sampled_up, preferred_element_type=jnp.float32)
    hidden = jnp.square(jax.nn.relu(before)).astype(jnp.bfloat16)
    prompt_out = jnp.dot(hidden, sampled_down, preferred_element_type=jnp.float32).astype(jnp.bfloat16)
    return (prompt_out, sampled_up, sampled_down)
```

```python
import functools

import jax
import jax.numpy as jnp
from jax import lax
from jax.experimental import pallas as pl
from jax.experimental.pallas import tpu as pltpu
from jax.sharding import PartitionSpec as P

MESH = pl.DeviceIdType.MESH
BF16 = jnp.bfloat16
F32 = jnp.float32


def kernel(
    nz, nx, tok_hbm, upm_hbm, dnm_hbm, gain_hbm, out_ref, upt_ref, dn_ref,
    tok, upm, dnm, gain, stage, slots, up, dn, nrm, dnt, upt, acc, ht, terms, rs_out, rs_in, outb,
    in_sem, xa_send, xa_recv, dy_send, dy_recv, zs_send, zs_recv, y_send, y_recv, x_send, x_recv, dn_send, dn_recv,
    rs_send, rs_recv, o_send, o_recv, l_sem,
):
    g, fs, x = lax.axis_index("grp"), lax.axis_index("fs"), lax.axis_index("tp")
    z, c = fs // 2, fs % 2
    par = g % 2
    other = g + 1 - 2 * par
    main = c == par
    agent = c != par
    adds = c == 1
    apart = jnp.logical_and(main, c == 0)
    right, left = (x + 1) % nx, (x + nx - 1) % nx
    per_col = nz // nx
    quarter = z // per_col
    shift = (nx - 1) - z % nx
    served = (x + nx - shift) % nx
    residue = (2 * nx - 1 - x + quarter) % nx
    far = (x + 2) % nx
    half = nz // 2
    rows = upm.shape[0]
    hid = dnm.shape[0]
    dcols = dnm.shape[1]
    wide = 2 * hid
    feat = 2 * rows

    def dev(g_, z_, c_, x_):
        return {"grp": g_, "fs": 2 * z_ + c_, "tp": x_}

    def remote(src, dst, ssem, rsem, to):
        return pltpu.make_async_remote_copy(
            src_ref=src, dst_ref=dst, send_sem=ssem, recv_sem=rsem, device_id=to, device_id_type=MESH
        )

    def up_rows(zs, cs):
        return up.at[pl.ds(pl.multiple_of((2 * zs + cs) * rows, 16), rows), :]

    def dn_part(h, xs):
        return dn.at[pl.ds(h * hid, hid), pl.ds(pl.multiple_of(xs * dcols, 128), dcols)]

    loads = [
        pltpu.make_async_copy(upm_hbm, upm, in_sem.at[0]),
        pltpu.make_async_copy(gain_hbm, gain, in_sem.at[1]),
        pltpu.make_async_copy(dnm_hbm, dnm, in_sem.at[2]),
        pltpu.make_async_copy(tok_hbm, tok, in_sem.at[3]),
    ]
    for k in range(4):
        loads[k].start()

    barrier = pltpu.get_barrier_semaphore()

    def greet(to):
        pl.semaphore_signal(barrier, inc=1, device_id=to, device_id_type=MESH)

    @pl.when(main)
    def _():
        def greet_agent(i, carry):
            greet(dev(g, i * nx + residue, 1 - par, x))
            return carry

        lax.fori_loop(0, per_col, greet_agent, 0)
        for to_x in (right, left):
            greet(dev(g, z, par, to_x))
        greet(dev(g, z, 1 - par, x))
        greet(dev(other, z, 1 - par, x))

    @pl.when(agent)
    def _():
        greet(dev(g, z, par, x))
        greet(dev(g, z, par, served))

    @pl.when(adds)
    def _():
        for d in (1, 2, nz - 1, nz - 2):
            greet(dev(g, (z + d) % nz, 1, x))

    loads[0].wait()
    loads[1].wait()

    @pl.when(main)
    def _():
        eye = lax.broadcasted_iota(jnp.int32, (rows, rows), 0) == lax.broadcasted_iota(jnp.int32, (rows, rows), 1)
        scale = jnp.sum(jnp.where(eye, gain[...], 0.0), axis=1, keepdims=True)
        stage[...] = (scale * upm[...]).astype(BF16)

    loads[2].wait()

    @pl.when(main)
    def _():
        dn_part(par, x)[...] = dnm[...].astype(BF16)

    peers = jnp.where(main, 5, 1 + per_col) + jnp.where(adds, 4, 0)
    pl.semaphore_wait(barrier, peers)

    rows_copy = remote(stage, slots, xa_send.at[0], xa_recv.at[0], dev(g, z, 1 - par, (x + shift) % nx))

    @pl.when(main)
    def _():
        rows_copy.start()

    def scatter_copy(j):
        part = slots.at[:, pl.ds(pl.multiple_of(j * wide, 128), wide)]
        return remote(
            part, up_rows(z, par), zs_send.at[j], zs_recv.at[z // nx], dev(g, per_col * served + j, par, x)
        )

    @pl.when(agent)
    def _():
        rows_copy.wait_recv()

        def scatter(k, carry):
            scatter_copy(k).start()
            return carry

        lax.fori_loop(0, per_col, scatter, 0)

    def to_mate(src, dst, k):
        return remote(src, dst, o_send.at[k], o_recv.at[k], dev(g, z, 1 - c, x))

    def half_of(ref, core, size):
        return ref.at[pl.ds(pl.multiple_of(core * size, 16), size), :]

    up_copy = to_mate(half_of(upt, 1 - par, hid), upt_ref, 0)
    dn_copy = to_mate(half_of(dn, 1 - par, hid), dn_ref, 1)
    out_copy = to_mate(outb.at[pl.ds(0, rows), :], out_ref, 2)
    dnt_copy = to_mate(dnt, dnt, 3)
    ht_copy = to_mate(ht, ht, 4)

    part_rows = hid // 2

    def down_part(xs, k):
        first = pl.multiple_of(par * hid + k * part_rows, 16)
        return dn.at[pl.ds(first, part_rows), pl.ds(pl.multiple_of(xs * dcols, 128), dcols)]

    def down_copy(xs, k, d, relayed):
        part = down_part(xs, k)
        return remote(
            part, part, dn_send.at[d, k, relayed], dn_recv.at[d, k, relayed], dev(g, z, par, left if d else right)
        )

    def down_across(xs, k, mine):
        part = dn_part(par if mine else 1 - par, xs)
        return remote(part, part, dy_send.at[k], dy_recv.at[k], dev(other, z, 1 - par, x))

    def piece(xs, k, i):
        cs = par if k == 0 else 1 - par
        return up_rows(nx * i + (2 * nx - 1 - xs + quarter) % nx, cs)

    def x_copy(xs, k, i, slot, to_right):
        d = 0 if to_right else 1
        part = piece(xs, k, i)
        return remote(part, part, x_send.at[d, slot], x_recv.at[d, slot], dev(g, z, par, right if to_right else left))

    def y_copy(i, mine):
        part = piece(x, 0 if mine else 1, i)
        return remote(part, part, y_send.at[i], y_recv.at[i], dev(other, z, 1 - par, x))

    def relay_slot(k, i):
        return 2 * per_col + k * (per_col // 2) + i // 2

    def relay(k, i):

        @pl.when(i % 2 == 0)
        def _():
            x_copy(left, k, i, k * per_col + i, True).wait_recv()
            x_copy(left, k, i, relay_slot(k, i), True).start()

        @pl.when(i % 2 == 1)
        def _():
            x_copy(right, k, i, k * per_col + i, False).wait_recv()
            x_copy(right, k, i, relay_slot(k, i), False).start()

    @pl.when(main)
    def _():
        for k in range(2):
            down_copy(x, k, 0, 0).start()
            down_copy(x, 1 - k, 1, 0).start()
        down_across(x, 0, True).start()

        loads[3].wait()
        block = 64

        def norm(b, carry):
            sl = pl.ds(pl.multiple_of(b * block, block), block)
            values = tok[sl, :].astype(F32)
            center = jnp.mean(values, axis=-1, keepdims=True)
            spread = jnp.mean(jnp.square(values - center), axis=-1, keepdims=True)
            nrm[sl, :] = ((values - center) * lax.rsqrt(spread + 1e-05)).astype(BF16)
            return carry

        lax.fori_loop(0, tok.shape[0] // block, norm, 0)

        down_copy(left, 0, 0, 0).wait_recv()
        down_copy(left, 0, 0, 1).start()
        down_copy(right, 1, 1, 0).wait_recv()
        down_copy(right, 1, 1, 1).start()
        down_copy(left, 1, 0, 0).wait_recv()
        down_across(left, 1, True).start()
        down_copy(right, 0, 1, 0).wait_recv()
        down_across(right, 2, True).start()

        def turn_down(j, carry):
            sl = pl.ds(pl.multiple_of(j * 128, 128), 128)
            dnt[sl, :] = dn[:, sl].T
            return carry

        own_dn = pltpu.make_async_copy(half_of(dn, par, hid), dn_ref, l_sem.at[0])

        def ordered(s):
            near_first = jnp.where(s % 2 == 0, per_col - 1 - s // 2, s // 2)
            return jnp.where(quarter == nx - 1, near_first, (s + 1) % per_col)

        chunk = nx * feat
        acc[...] = jnp.zeros_like(acc)

        def at_lag(s, lag, run):
            @pl.when(jnp.logical_and(s >= lag, s < per_col + lag))
            def _():
                run(ordered(s - lag))

        def arrived(i):
            remote(piece(x, 0, i), piece(x, 0, i), y_send.at[0], zs_recv.at[i], dev(other, z, 1 - par, x)).wait_recv()
            y_copy(i, True).start()
            x_copy(x, 0, i, i, True).start()
            x_copy(x, 0, i, i, False).start()

        def crossed(i):
            y_copy(i, False).wait_recv()
            x_copy(x, 1, i, per_col + i, True).start()
            x_copy(x, 1, i, per_col + i, False).start()
            relay(0, i)

        def complete(i):
            for k in range(2):

                @pl.when(i % 2 == 1)
                def _():
                    x_copy(left, k, i, k * per_col + i, True).wait_recv()
                    x_copy(far, k, i, relay_slot(k, i), False).wait_recv()

                @pl.when(i % 2 == 0)
                def _():
                    x_copy(right, k, i, k * per_col + i, False).wait_recv()
                    x_copy(far, k, i, relay_slot(k, i), True).wait_recv()

            sl = pl.ds(pl.multiple_of(i * chunk, 128), chunk)
            acc[...] += jnp.dot(nrm[:, sl], up[sl, :], preferred_element_type=F32)

        def gather_up(s, carry):
            @pl.when(s == 1)
            def _():
                down_copy(far, 0, 0, 1).wait_recv()
                down_copy(far, 1, 1, 1).wait_recv()
                down_across(far, 3, True).start()

            at_lag(s, 0, arrived)
            at_lag(s, 2, crossed)
            at_lag(s, 4, lambda i: relay(1, i))

            @pl.when(s == per_col)
            def _():
                for k, xs in enumerate((x, left, right, far)):
                    down_across(xs, k, False).wait_recv()
                own_dn.start()
                dn_copy.start()
                lax.fori_loop(0, dn.shape[1] // 128, turn_down, 0)

                @pl.when(apart)
                def _():
                    dnt_copy.start()

            at_lag(s, 5, complete)
            return carry

        lax.fori_loop(0, per_col + 5, gather_up, 0)

        ht[...] = jnp.square(jnp.maximum(acc[...], 0.0)).T.astype(BF16)

        @pl.when(apart)
        def _():
            ht_copy.start()

    def turn_up(j, carry):
        sl = pl.ds(pl.multiple_of(j * 128, 128), 128)
        upt[:, sl] = up[sl, :].T
        return carry

    turns = up.shape[0] // 128
    own_up = pltpu.make_async_copy(half_of(upt, par, hid), upt_ref, l_sem.at[1])
    own_out = pltpu.make_async_copy(outb.at[pl.ds(rows, rows), :], out_ref, l_sem.at[2])

    @pl.when(apart)
    def _():
        lax.fori_loop(0, turns, turn_up, 0)
        up_copy.start()
        own_up.start()

    @pl.when(jnp.logical_and(agent, adds))
    def _():
        dnt_copy.wait_recv()
        ht_copy.wait_recv()

    @pl.when(adds)
    def _():
        chains = ((1, 0), (1, 1), (-1, 1), (-1, 0))

        def rs_copy(ch, s, sub, dist):
            sign = chains[ch][0]
            to = (z + nz + sign * dist) % nz
            return remote(
                rs_out.at[ch, s, sub], rs_in.at[ch, s, sub], rs_send.at[ch, s, sub], rs_recv.at[ch, s, sub], dev(g, to, 1, x)
            )

        def rows_of(zt, sub):
            return pl.ds(pl.multiple_of(zt * feat + sub * rows, 16), rows)

        def step(s, skip, first_of):
            for sub in range(2):
                for ch in (1, 2, 0, 3):
                    if ch in skip:
                        continue
                    sign, odd = chains[ch]
                    d = half - odd - 2 * s
                    sl = rows_of((z + 2 * nz + sign * d) % nz, sub)
                    if isinstance(s, int) and s == 0:
                        value = jnp.dot(dnt[sl, :], ht[...], preferred_element_type=F32)
                    else:
                        value = terms[sl, :]
                    if ch not in first_of:
                        rs_copy(ch, s - 1, sub, 2).wait_recv()
                        value = value + rs_in[ch, s - 1, sub].astype(F32)
                    rs_out[ch, s, sub] = value.astype(BF16)
                    rs_copy(ch, s, sub, jnp.minimum(d, 2)).start()

        def turn_some(s):
            @pl.when(main)
            def _():
                lax.fori_loop(4 * s, jnp.minimum(4 * s + 4, turns), turn_up, 0)

        tc = 512

        def all_terms(b, carry):
            sl = pl.ds(pl.multiple_of(b * tc, tc), tc)
            terms[sl, :] = jnp.dot(dnt[sl, :], ht[...], preferred_element_type=F32)
            return carry

        steps = half // 2
        step(0, (3,), (0, 1, 2))
        lax.fori_loop(0, terms.shape[0] // tc, all_terms, 0)
        turn_some(0)
        step(1, (), (3,))
        turn_some(1)

        def steady(s, carry):
            step(s, (), ())

            turn_some(s)
            return carry

        lax.fori_loop(2, steps, steady, 0)
        @pl.when(main)
        def _():
            up_copy.start()
            own_up.start()

        for sub in range(2):
            total = terms[rows_of(z, sub), :]
            for ch in range(4):
                rs_copy(ch, steps - 1, sub, 2).wait_recv()
                total = total + rs_in[ch, steps - 1, sub].astype(F32)
            outb[pl.ds(sub * rows, rows), :] = total.astype(BF16)
        out_copy.start()
        own_out.start()

        def rs_sent(s, carry):
            for sub in range(2):
                for ch in range(3):
                    rs_copy(ch, s, sub, 2).wait_send()

                @pl.when(s > 0)
                def _():
                    rs_copy(3, s, sub, 2).wait_send()

            return carry

        lax.fori_loop(0, steps, rs_sent, 0)
        out_copy.wait_send()
        own_out.wait()

    @pl.when(main)
    def _():
        rows_copy.wait_send()
        down_copy(left, 0, 0, 1).wait_send()
        down_copy(right, 1, 1, 1).wait_send()
        for d in range(2):
            for k in range(2):
                down_copy(x, k, d, 0).wait_send()
        for k, xs in enumerate((x, left, right, far)):
            down_across(xs, k, True).wait_send()

        def sent(i, carry):
            y_copy(i, True).wait_send()
            for k in range(2):
                x_copy(x, k, i, k * per_col + i, True).wait_send()
                x_copy(x, k, i, k * per_col + i, False).wait_send()

                @pl.when(i % 2 == 0)
                def _():
                    x_copy(left, k, i, relay_slot(k, i), True).wait_send()

                @pl.when(i % 2 == 1)
                def _():
                    x_copy(right, k, i, relay_slot(k, i), False).wait_send()

            return carry

        lax.fori_loop(0, per_col, sent, 0)
        dn_copy.wait_send()
        up_copy.wait_send()
        own_dn = pltpu.make_async_copy(half_of(dn, par, hid), dn_ref, l_sem.at[0])
        own_dn.wait()
        own_up.wait()

    @pl.when(apart)
    def _():
        dnt_copy.wait_send()
        ht_copy.wait_send()

    @pl.when(agent)
    def _():
        loads[3].wait()
        dn_copy.wait_recv()
        up_copy.wait_recv()

    @pl.when(c == 0)
    def _():
        out_copy.wait_recv()

    @pl.when(agent)
    def _():
        def scattered(j, carry):
            scatter_copy(j).wait_send()
            return carry

        lax.fori_loop(0, per_col, scattered, 0)


def result_kernel(*refs):
    sources, results, buffers, (in_sem, out_sem) = refs[:3], refs[3:6], refs[6:9], refs[9:]
    reads, writes = [], []
    for k in range(3):
        size = sources[k].shape[0] // 2 // 16 * 16
        for part, sl in enumerate((pl.ds(0, size), pl.ds(size, sources[k].shape[0] - size))):
            reads.append(pltpu.make_async_copy(sources[k].at[sl], buffers[k].at[sl], in_sem.at[k, part]))
            writes.append(pltpu.make_async_copy(buffers[k].at[sl], results[k].at[sl], out_sem.at[k, part]))
    for read in reads:
        read.start()
    for read, write in zip(reads, writes):
        read.wait()
        write.start()
    for write in writes:
        write.wait()


def solution(mesh):
    nz, nx = mesh.shape["fs"] // 2, mesh.shape["tp"]

    def shards(tokens, up_master, down_master, norm_gain):
        rows = up_master.shape[0]
        hid, dcols = down_master.shape
        count, width = tokens.shape
        feat, wide = 2 * rows, 2 * hid
        steps = nz // 4
        per_col = nz // nx
        dma = pltpu.SemaphoreType.DMA
        any_space = pl.BlockSpec(memory_space=pltpu.HBM)
        results = pl.pallas_call(
            functools.partial(kernel, nz, nx),
            out_shape=(
                jax.ShapeDtypeStruct((rows, count), BF16),
                jax.ShapeDtypeStruct((hid, width), BF16),
                jax.ShapeDtypeStruct((hid, width), BF16),
            ),
            in_specs=[any_space] * 4,
            out_specs=(any_space,) * 3,
            scratch_shapes=[
                pltpu.VMEM((count, width), BF16),
                pltpu.VMEM(up_master.shape, F32),
                pltpu.VMEM(down_master.shape, F32),
                pltpu.VMEM((1, rows), F32),
                pltpu.VMEM(up_master.shape, BF16),
                pltpu.VMEM(up_master.shape, BF16),
                pltpu.VMEM((width, wide), BF16),
                pltpu.VMEM((wide, width), BF16),
                pltpu.VMEM((count, width), BF16),
                pltpu.VMEM((width, wide), BF16),
                pltpu.VMEM((wide, width), BF16),
                pltpu.VMEM((count, wide), F32),
                pltpu.VMEM((wide, count), BF16),
                pltpu.VMEM((width, count), F32),
                pltpu.VMEM((4, steps, 2, rows, count), BF16),
                pltpu.VMEM((4, steps, 2, rows, count), BF16),
                pltpu.VMEM((feat, count), BF16),
                dma((4,)),
                dma((1,)),
                dma((1,)),
                dma((4,)),
                dma((4,)),
                dma((per_col,)),
                dma((per_col,)),
                dma((per_col,)),
                dma((per_col,)),
                dma((2, 3 * per_col)),
                dma((2, 3 * per_col)),
                dma((2, 2, 2)),
                dma((2, 2, 2)),
                dma((4, steps, 2)),
                dma((4, steps, 2)),
                dma((5,)),
                dma((5,)),
                dma((3,)),
            ],
            compiler_params=pltpu.CompilerParams(
                collective_id=0, has_side_effects=True, vmem_limit_bytes=60 * 1024 * 1024
            ),
        )(tokens, up_master, down_master, norm_gain[None])
        out_t, up_t, down = pl.pallas_call(
            result_kernel,
            out_shape=tuple(jax.ShapeDtypeStruct(r.shape, r.dtype) for r in results),
            in_specs=[any_space] * 3,
            out_specs=(any_space,) * 3,
            scratch_shapes=[pltpu.VMEM(r.shape, r.dtype) for r in results] + [dma((3, 2)), dma((3, 2))],
            compiler_params=pltpu.CompilerParams(vmem_limit_bytes=60 * 1024 * 1024),
        )(*results)
        return out_t.T, up_t.T, down

    return jax.shard_map(
        shards,
        mesh=mesh,
        in_specs=(P(("grp", "tp"), None), P("fs", "tp"), P("fs", "tp"), P("fs")),
        out_specs=(P(("grp", "tp"), "fs"), P("grp", "fs"), P(("grp", "fs"), None)),
        check_vma=False,
    )
```

```python
import functools

import jax
import jax.numpy as jnp
from jax import lax
from jax.experimental import pallas as pl
from jax.experimental.pallas import tpu as pltpu
from jax.sharding import PartitionSpec as P

MESH = pl.DeviceIdType.MESH
BF16 = jnp.bfloat16
F32 = jnp.float32


def kernel(
    nz, nx, tok_hbm, upm_hbm, dnm_hbm, gain_hbm, out_ref, upt_ref, dn_ref,
    tok, upm, dnm, gain, stage, slots, up, dn, nrm, dnt, upt, acc, ht, terms, rs_out, rs_in, outb,
    in_sem, xa_send, xa_recv, dy_send, dy_recv, zs_send, zs_recv, y_send, y_recv, x_send, x_recv, dn_send, dn_recv,
    rs_send, rs_recv, o_send, o_recv, l_sem,
):
    g, fs, x = lax.axis_index("grp"), lax.axis_index("fs"), lax.axis_index("tp")
    z, c = fs // 2, fs % 2
    par = g % 2
    other = g + 1 - 2 * par
    main = c == par
    agent = c != par
    adds = c == 1
    apart = jnp.logical_and(main, c == 0)
    right, left = (x + 1) % nx, (x + nx - 1) % nx
    per_col = nz // nx
    quarter = z // per_col
    shift = (nx - 1) - z % nx
    served = (x + nx - shift) % nx
    residue = (2 * nx - 1 - x + quarter) % nx
    far = (x + 2) % nx
    half = nz // 2
    rows = upm.shape[0]
    hid = dnm.shape[0]
    dcols = dnm.shape[1]
    wide = 2 * hid
    feat = 2 * rows

    def dev(g_, z_, c_, x_):
        return {"grp": g_, "fs": 2 * z_ + c_, "tp": x_}

    def remote(src, dst, ssem, rsem, to):
        return pltpu.make_async_remote_copy(
            src_ref=src, dst_ref=dst, send_sem=ssem, recv_sem=rsem, device_id=to, device_id_type=MESH
        )

    def up_rows(zs, cs):
        return up.at[pl.ds(pl.multiple_of((2 * zs + cs) * rows, 16), rows), :]

    def dn_part(h, xs):
        return dn.at[pl.ds(h * hid, hid), pl.ds(pl.multiple_of(xs * dcols, 128), dcols)]

    loads = [
        pltpu.make_async_copy(upm_hbm, upm, in_sem.at[0]),
        pltpu.make_async_copy(gain_hbm, gain, in_sem.at[1]),
        pltpu.make_async_copy(dnm_hbm, dnm, in_sem.at[2]),
        pltpu.make_async_copy(tok_hbm, tok, in_sem.at[3]),
    ]
    for k in range(4):
        loads[k].start()

    barrier = pltpu.get_barrier_semaphore()

    def greet(to):
        pl.semaphore_signal(barrier, inc=1, device_id=to, device_id_type=MESH)

    @pl.when(main)
    def _():
        def greet_agent(i, carry):
            greet(dev(g, i * nx + residue, 1 - par, x))
            return carry

        lax.fori_loop(0, per_col, greet_agent, 0)
        for to_x in (right, left):
            greet(dev(g, z, par, to_x))
        greet(dev(g, z, 1 - par, x))
        greet(dev(other, z, 1 - par, x))

    @pl.when(agent)
    def _():
        greet(dev(g, z, par, x))
        greet(dev(g, z, par, served))

    @pl.when(adds)
    def _():
        for d in (1, 2, nz - 1, nz - 2):
            greet(dev(g, (z + d) % nz, 1, x))

    loads[0].wait()
    loads[1].wait()

    @pl.when(main)
    def _():
        eye = lax.broadcasted_iota(jnp.int32, (rows, rows), 0) == lax.broadcasted_iota(jnp.int32, (rows, rows), 1)
        scale = jnp.sum(jnp.where(eye, gain[...], 0.0), axis=1, keepdims=True)
        stage[...] = (scale * upm[...]).astype(BF16)

    loads[2].wait()

    @pl.when(main)
    def _():
        dn_part(par, x)[...] = dnm[...].astype(BF16)

    peers = jnp.where(main, 5, 1 + per_col) + jnp.where(adds, 4, 0)
    pl.semaphore_wait(barrier, peers)

    rows_copy = remote(stage, slots, xa_send.at[0], xa_recv.at[0], dev(g, z, 1 - par, (x + shift) % nx))

    @pl.when(main)
    def _():
        rows_copy.start()

    def scatter_copy(j):
        part = slots.at[:, pl.ds(pl.multiple_of(j * wide, 128), wide)]
        return remote(
            part, up_rows(z, par), zs_send.at[j], zs_recv.at[z // nx], dev(g, per_col * served + j, par, x)
        )

    @pl.when(agent)
    def _():
        rows_copy.wait_recv()

        def scatter(k, carry):
            scatter_copy(k).start()
            return carry

        lax.fori_loop(0, per_col, scatter, 0)

    def to_mate(src, dst, k):
        return remote(src, dst, o_send.at[k], o_recv.at[k], dev(g, z, 1 - c, x))

    def half_of(ref, core, size):
        return ref.at[pl.ds(pl.multiple_of(core * size, 16), size), :]

    up_copy = to_mate(half_of(upt, 1 - par, hid), upt_ref, 0)
    dn_copy = to_mate(half_of(dn, 1 - par, hid), dn_ref, 1)
    out_copy = to_mate(outb.at[pl.ds(0, rows), :], out_ref, 2)
    dnt_copy = to_mate(dnt, dnt, 3)
    ht_copy = to_mate(ht, ht, 4)

    part_rows = hid // 2

    def down_part(xs, k):
        first = pl.multiple_of(par * hid + k * part_rows, 16)
        return dn.at[pl.ds(first, part_rows), pl.ds(pl.multiple_of(xs * dcols, 128), dcols)]

    def down_copy(xs, k, d, relayed):
        part = down_part(xs, k)
        return remote(
            part, part, dn_send.at[d, k, relayed], dn_recv.at[d, k, relayed], dev(g, z, par, left if d else right)
        )

    def down_across(xs, k, mine):
        part = dn_part(par if mine else 1 - par, xs)
        return remote(part, part, dy_send.at[k], dy_recv.at[k], dev(other, z, 1 - par, x))

    def piece(xs, k, i):
        cs = par if k == 0 else 1 - par
        return up_rows(nx * i + (2 * nx - 1 - xs + quarter) % nx, cs)

    def x_copy(xs, k, i, slot, to_right):
        d = 0 if to_right else 1
        part = piece(xs, k, i)
        return remote(part, part, x_send.at[d, slot], x_recv.at[d, slot], dev(g, z, par, right if to_right else left))

    def y_copy(i, mine):
        part = piece(x, 0 if mine else 1, i)
        return remote(part, part, y_send.at[i], y_recv.at[i], dev(other, z, 1 - par, x))

    def relay_slot(k, i):
        return 2 * per_col + k * (per_col // 2) + i // 2

    def relay(k, i):

        @pl.when(i % 2 == 0)
        def _():
            x_copy(left, k, i, k * per_col + i, True).wait_recv()
            x_copy(left, k, i, relay_slot(k, i), True).start()

        @pl.when(i % 2 == 1)
        def _():
            x_copy(right, k, i, k * per_col + i, False).wait_recv()
            x_copy(right, k, i, relay_slot(k, i), False).start()

    @pl.when(main)
    def _():
        for k in range(2):
            down_copy(x, k, 0, 0).start()
            down_copy(x, 1 - k, 1, 0).start()
        down_across(x, 0, True).start()

        loads[3].wait()
        block = 64

        def norm(b, carry):
            sl = pl.ds(pl.multiple_of(b * block, block), block)
            values = tok[sl, :].astype(F32)
            center = jnp.mean(values, axis=-1, keepdims=True)
            spread = jnp.mean(jnp.square(values - center), axis=-1, keepdims=True)
            nrm[sl, :] = ((values - center) * lax.rsqrt(spread + 1e-05)).astype(BF16)
            return carry

        lax.fori_loop(0, tok.shape[0] // block, norm, 0)

        down_copy(left, 0, 0, 0).wait_recv()
        down_copy(left, 0, 0, 1).start()
        down_copy(right, 1, 1, 0).wait_recv()
        down_copy(right, 1, 1, 1).start()
        down_copy(left, 1, 0, 0).wait_recv()
        down_across(left, 1, True).start()
        down_copy(right, 0, 1, 0).wait_recv()
        down_across(right, 2, True).start()

        def turn_down(j, carry):
            sl = pl.ds(pl.multiple_of(j * 128, 128), 128)
            dnt[sl, :] = dn[:, sl].T
            return carry

        own_dn = pltpu.make_async_copy(half_of(dn, par, hid), dn_ref, l_sem.at[0])

        def ordered(s):
            away = (s + 1) // 2
            near_first = (z // nx + per_col + jnp.where(s % 2 == 1, away, -away)) % per_col
            return jnp.where(quarter < nx // 2, (s + 1) % per_col, near_first)

        chunk = nx * feat
        acc[...] = jnp.zeros_like(acc)

        def at_lag(s, lag, run):
            @pl.when(jnp.logical_and(s >= lag, s < per_col + lag))
            def _():
                run(ordered(s - lag))

        def arrived(i):
            remote(piece(x, 0, i), piece(x, 0, i), y_send.at[0], zs_recv.at[i], dev(other, z, 1 - par, x)).wait_recv()
            y_copy(i, True).start()
            x_copy(x, 0, i, i, True).start()
            x_copy(x, 0, i, i, False).start()

        def crossed(i):
            y_copy(i, False).wait_recv()
            x_copy(x, 1, i, per_col + i, True).start()
            x_copy(x, 1, i, per_col + i, False).start()

        def complete(i):
            for k in range(2):

                @pl.when(i % 2 == 1)
                def _():
                    x_copy(left, k, i, k * per_col + i, True).wait_recv()
                    x_copy(far, k, i, relay_slot(k, i), False).wait_recv()

                @pl.when(i % 2 == 0)
                def _():
                    x_copy(right, k, i, k * per_col + i, False).wait_recv()
                    x_copy(far, k, i, relay_slot(k, i), True).wait_recv()

            sl = pl.ds(pl.multiple_of(i * chunk, 128), chunk)
            acc[...] += jnp.dot(nrm[:, sl], up[sl, :], preferred_element_type=F32)

        def gather_up(s, carry):
            @pl.when(s == 1)
            def _():
                down_copy(far, 0, 0, 1).wait_recv()
                down_copy(far, 1, 1, 1).wait_recv()
                down_across(far, 3, True).start()

            at_lag(s, 0, arrived)
            at_lag(s, 2, crossed)
            at_lag(s, 3, lambda i: relay(0, i))
            at_lag(s, 5, lambda i: relay(1, i))

            @pl.when(s == per_col)
            def _():
                for k, xs in enumerate((x, left, right, far)):
                    down_across(xs, k, False).wait_recv()
                own_dn.start()
                dn_copy.start()
                lax.fori_loop(0, dn.shape[1] // 128, turn_down, 0)

                @pl.when(apart)
                def _():
                    dnt_copy.start()

            at_lag(s, 7, complete)
            return carry

        lax.fori_loop(0, per_col + 7, gather_up, 0)

        ht[...] = jnp.square(jnp.maximum(acc[...], 0.0)).T.astype(BF16)

        @pl.when(apart)
        def _():
            ht_copy.start()

    def turn_up(j, carry):
        sl = pl.ds(pl.multiple_of(j * 128, 128), 128)
        upt[:, sl] = up[sl, :].T
        return carry

    turns = up.shape[0] // 128
    own_up = pltpu.make_async_copy(half_of(upt, par, hid), upt_ref, l_sem.at[1])
    own_out = pltpu.make_async_copy(outb.at[pl.ds(rows, rows), :], out_ref, l_sem.at[2])

    @pl.when(apart)
    def _():
        lax.fori_loop(0, turns, turn_up, 0)
        up_copy.start()
        own_up.start()

    @pl.when(jnp.logical_and(agent, adds))
    def _():
        dnt_copy.wait_recv()
        ht_copy.wait_recv()

    @pl.when(adds)
    def _():
        chains = ((1, 0), (1, 1), (-1, 1), (-1, 0))

        def rs_copy(ch, s, sub, dist):
            sign = chains[ch][0]
            to = (z + nz + sign * dist) % nz
            return remote(
                rs_out.at[ch, s, sub], rs_in.at[ch, s, sub], rs_send.at[ch, s, sub], rs_recv.at[ch, s, sub], dev(g, to, 1, x)
            )

        def rows_of(zt, sub):
            return pl.ds(pl.multiple_of(zt * feat + sub * rows, 16), rows)

        def step(s, skip, first_of):
            for sub in range(2):
                for ch in (1, 2, 0, 3):
                    if ch in skip:
                        continue
                    sign, odd = chains[ch]
                    d = half - odd - 2 * s
                    sl = rows_of((z + 2 * nz + sign * d) % nz, sub)
                    if isinstance(s, int) and s == 0:
                        value = jnp.dot(dnt[sl, :], ht[...], preferred_element_type=F32)
                    else:
                        value = terms[sl, :]
                    if ch not in first_of:
                        rs_copy(ch, s - 1, sub, 2).wait_recv()
                        value = value + rs_in[ch, s - 1, sub].astype(F32)
                    rs_out[ch, s, sub] = value.astype(BF16)
                    rs_copy(ch, s, sub, jnp.minimum(d, 2)).start()

        def turn_some(s):
            @pl.when(main)
            def _():
                lax.fori_loop(4 * s, jnp.minimum(4 * s + 4, turns), turn_up, 0)

        tc = 512

        def all_terms(b, carry):
            sl = pl.ds(pl.multiple_of(b * tc, tc), tc)
            terms[sl, :] = jnp.dot(dnt[sl, :], ht[...], preferred_element_type=F32)
            return carry

        steps = half // 2
        step(0, (3,), (0, 1, 2))
        lax.fori_loop(0, terms.shape[0] // tc, all_terms, 0)
        turn_some(0)
        step(1, (), (3,))
        turn_some(1)

        def steady(s, carry):
            step(s, (), ())

            turn_some(s)
            return carry

        lax.fori_loop(2, steps, steady, 0)
        @pl.when(main)
        def _():
            up_copy.start()
            own_up.start()

        for sub in range(2):
            total = terms[rows_of(z, sub), :]
            for ch in range(4):
                rs_copy(ch, steps - 1, sub, 2).wait_recv()
                total = total + rs_in[ch, steps - 1, sub].astype(F32)
            outb[pl.ds(sub * rows, rows), :] = total.astype(BF16)
        out_copy.start()
        own_out.start()

        def rs_sent(s, carry):
            for sub in range(2):
                for ch in range(3):
                    rs_copy(ch, s, sub, 2).wait_send()

                @pl.when(s > 0)
                def _():
                    rs_copy(3, s, sub, 2).wait_send()

            return carry

        lax.fori_loop(0, steps, rs_sent, 0)
        out_copy.wait_send()
        own_out.wait()

    @pl.when(main)
    def _():
        rows_copy.wait_send()
        down_copy(left, 0, 0, 1).wait_send()
        down_copy(right, 1, 1, 1).wait_send()
        for d in range(2):
            for k in range(2):
                down_copy(x, k, d, 0).wait_send()
        for k, xs in enumerate((x, left, right, far)):
            down_across(xs, k, True).wait_send()

        def sent(i, carry):
            y_copy(i, True).wait_send()
            for k in range(2):
                x_copy(x, k, i, k * per_col + i, True).wait_send()
                x_copy(x, k, i, k * per_col + i, False).wait_send()

                @pl.when(i % 2 == 0)
                def _():
                    x_copy(left, k, i, relay_slot(k, i), True).wait_send()

                @pl.when(i % 2 == 1)
                def _():
                    x_copy(right, k, i, relay_slot(k, i), False).wait_send()

            return carry

        lax.fori_loop(0, per_col, sent, 0)
        dn_copy.wait_send()
        up_copy.wait_send()
        own_dn = pltpu.make_async_copy(half_of(dn, par, hid), dn_ref, l_sem.at[0])
        own_dn.wait()
        own_up.wait()

    @pl.when(apart)
    def _():
        dnt_copy.wait_send()
        ht_copy.wait_send()

    @pl.when(agent)
    def _():
        loads[3].wait()
        dn_copy.wait_recv()
        up_copy.wait_recv()

    @pl.when(c == 0)
    def _():
        out_copy.wait_recv()

    @pl.when(agent)
    def _():
        def scattered(j, carry):
            scatter_copy(j).wait_send()
            return carry

        lax.fori_loop(0, per_col, scattered, 0)


def result_kernel(*refs):
    sources, results, buffers, (in_sem, out_sem) = refs[:3], refs[3:6], refs[6:9], refs[9:]
    reads, writes = [], []
    for k in range(3):
        size = sources[k].shape[0] // 2 // 16 * 16
        for part, sl in enumerate((pl.ds(0, size), pl.ds(size, sources[k].shape[0] - size))):
            reads.append(pltpu.make_async_copy(sources[k].at[sl], buffers[k].at[sl], in_sem.at[k, part]))
            writes.append(pltpu.make_async_copy(buffers[k].at[sl], results[k].at[sl], out_sem.at[k, part]))
    for read in reads:
        read.start()
    for read, write in zip(reads, writes):
        read.wait()
        write.start()
    for write in writes:
        write.wait()


def solution(mesh):
    nz, nx = mesh.shape["fs"] // 2, mesh.shape["tp"]

    def shards(tokens, up_master, down_master, norm_gain):
        rows = up_master.shape[0]
        hid, dcols = down_master.shape
        count, width = tokens.shape
        feat, wide = 2 * rows, 2 * hid
        steps = nz // 4
        per_col = nz // nx
        dma = pltpu.SemaphoreType.DMA
        any_space = pl.BlockSpec(memory_space=pltpu.HBM)
        results = pl.pallas_call(
            functools.partial(kernel, nz, nx),
            out_shape=(
                jax.ShapeDtypeStruct((rows, count), BF16),
                jax.ShapeDtypeStruct((hid, width), BF16),
                jax.ShapeDtypeStruct((hid, width), BF16),
            ),
            in_specs=[any_space] * 4,
            out_specs=(any_space,) * 3,
            scratch_shapes=[
                pltpu.VMEM((count, width), BF16),
                pltpu.VMEM(up_master.shape, F32),
                pltpu.VMEM(down_master.shape, F32),
                pltpu.VMEM((1, rows), F32),
                pltpu.VMEM(up_master.shape, BF16),
                pltpu.VMEM(up_master.shape, BF16),
                pltpu.VMEM((width, wide), BF16),
                pltpu.VMEM((wide, width), BF16),
                pltpu.VMEM((count, width), BF16),
                pltpu.VMEM((width, wide), BF16),
                pltpu.VMEM((wide, width), BF16),
                pltpu.VMEM((count, wide), F32),
                pltpu.VMEM((wide, count), BF16),
                pltpu.VMEM((width, count), F32),
                pltpu.VMEM((4, steps, 2, rows, count), BF16),
                pltpu.VMEM((4, steps, 2, rows, count), BF16),
                pltpu.VMEM((feat, count), BF16),
                dma((4,)),
                dma((1,)),
                dma((1,)),
                dma((4,)),
                dma((4,)),
                dma((per_col,)),
                dma((per_col,)),
                dma((per_col,)),
                dma((per_col,)),
                dma((2, 3 * per_col)),
                dma((2, 3 * per_col)),
                dma((2, 2, 2)),
                dma((2, 2, 2)),
                dma((4, steps, 2)),
                dma((4, steps, 2)),
                dma((5,)),
                dma((5,)),
                dma((3,)),
            ],
            compiler_params=pltpu.CompilerParams(
                collective_id=0, has_side_effects=True, vmem_limit_bytes=60 * 1024 * 1024
            ),
        )(tokens, up_master, down_master, norm_gain[None])
        out_t, up_t, down = pl.pallas_call(
            result_kernel,
            out_shape=tuple(jax.ShapeDtypeStruct(r.shape, r.dtype) for r in results),
            in_specs=[any_space] * 3,
            out_specs=(any_space,) * 3,
            scratch_shapes=[pltpu.VMEM(r.shape, r.dtype) for r in results] + [dma((3, 2)), dma((3, 2))],
            compiler_params=pltpu.CompilerParams(vmem_limit_bytes=60 * 1024 * 1024),
        )(*results)
        return out_t.T, up_t.T, down

    return jax.shard_map(
        shards,
        mesh=mesh,
        in_specs=(P(("grp", "tp"), None), P("fs", "tp"), P("fs", "tp"), P("fs")),
        out_specs=(P(("grp", "tp"), "fs"), P("grp", "fs"), P(("grp", "fs"), None)),
        check_vma=False,
    )
```

```python
import functools

import jax
import jax.numpy as jnp
from jax import lax
from jax.experimental import pallas as pl
from jax.experimental.pallas import tpu as pltpu
from jax.sharding import PartitionSpec as P

MESH = pl.DeviceIdType.MESH
BF16 = jnp.bfloat16
F32 = jnp.float32


def kernel(
    nz, nx, tok_hbm, upm_hbm, dnm_hbm, gain_hbm, out_ref, upt_ref, dn_ref,
    tok, upm, dnm, gain, stage, slots, up, dn, nrm, dnt, upt, acc, ht, terms, rs_out, rs_in, outb,
    in_sem, xa_send, xa_recv, dy_send, dy_recv, zs_send, zs_recv, y_send, y_recv, x_send, x_recv, dn_send, dn_recv,
    rs_send, rs_recv, o_send, o_recv, l_sem,
):
    g, fs, x = lax.axis_index("grp"), lax.axis_index("fs"), lax.axis_index("tp")
    z, c = fs // 2, fs % 2
    par = g % 2
    other = g + 1 - 2 * par
    main = c == par
    agent = c != par
    adds = c == 1
    apart = jnp.logical_and(main, c == 0)
    right, left = (x + 1) % nx, (x + nx - 1) % nx
    per_col = nz // nx
    quarter = z // per_col
    shift = (nx - 1) - z % nx
    served = (x + nx - shift) % nx
    residue = (2 * nx - 1 - x + quarter) % nx
    far = (x + 2) % nx
    half = nz // 2
    rows = upm.shape[0]
    hid = dnm.shape[0]
    dcols = dnm.shape[1]
    wide = 2 * hid
    feat = 2 * rows

    def dev(g_, z_, c_, x_):
        return {"grp": g_, "fs": 2 * z_ + c_, "tp": x_}

    def remote(src, dst, ssem, rsem, to):
        return pltpu.make_async_remote_copy(
            src_ref=src, dst_ref=dst, send_sem=ssem, recv_sem=rsem, device_id=to, device_id_type=MESH
        )

    def up_rows(zs, cs):
        return up.at[pl.ds(pl.multiple_of((2 * zs + cs) * rows, 16), rows), :]

    def dn_part(h, xs):
        return dn.at[pl.ds(h * hid, hid), pl.ds(pl.multiple_of(xs * dcols, 128), dcols)]

    loads = [
        pltpu.make_async_copy(upm_hbm, upm, in_sem.at[0]),
        pltpu.make_async_copy(gain_hbm, gain, in_sem.at[1]),
        pltpu.make_async_copy(dnm_hbm, dnm, in_sem.at[2]),
        pltpu.make_async_copy(tok_hbm, tok, in_sem.at[3]),
    ]
    for k in range(4):
        loads[k].start()

    barrier = pltpu.get_barrier_semaphore()

    def greet(to):
        pl.semaphore_signal(barrier, inc=1, device_id=to, device_id_type=MESH)

    @pl.when(main)
    def _():
        def greet_agent(i, carry):
            greet(dev(g, i * nx + residue, 1 - par, x))
            return carry

        lax.fori_loop(0, per_col, greet_agent, 0)
        for to_x in (right, left):
            greet(dev(g, z, par, to_x))
        greet(dev(g, z, 1 - par, x))
        greet(dev(other, z, 1 - par, x))

    @pl.when(agent)
    def _():
        greet(dev(g, z, par, x))
        greet(dev(g, z, par, served))

    @pl.when(adds)
    def _():
        for d in (1, 2, nz - 1, nz - 2):
            greet(dev(g, (z + d) % nz, 1, x))

    loads[0].wait()
    loads[1].wait()

    @pl.when(main)
    def _():
        eye = lax.broadcasted_iota(jnp.int32, (rows, rows), 0) == lax.broadcasted_iota(jnp.int32, (rows, rows), 1)
        scale = jnp.sum(jnp.where(eye, gain[...], 0.0), axis=1, keepdims=True)
        stage[...] = (scale * upm[...]).astype(BF16)

    loads[2].wait()

    @pl.when(main)
    def _():
        dn_part(par, x)[...] = dnm[...].astype(BF16)

    peers = jnp.where(main, 5, 1 + per_col) + jnp.where(adds, 4, 0)
    pl.semaphore_wait(barrier, peers)

    pieces = 4
    per_piece = per_col // pieces

    def rows_copy(k):
        sl = pl.ds(k * per_piece * wide, per_piece * wide)
        return remote(
            stage.at[:, sl], slots.at[:, sl], xa_send.at[k], xa_recv.at[k], dev(g, z, 1 - par, (x + shift) % nx)
        )

    @pl.when(main)
    def _():
        for k in range(pieces):
            rows_copy(k).start()

    def scatter_copy(j):
        part = slots.at[:, pl.ds(pl.multiple_of(j * wide, 128), wide)]
        return remote(
            part, up_rows(z, par), zs_send.at[j], zs_recv.at[z // nx], dev(g, per_col * served + j, par, x)
        )

    @pl.when(agent)
    def _():
        for k in range(pieces):
            rows_copy(k).wait_recv()
            for j in range(per_piece):
                scatter_copy(k * per_piece + j).start()

    def to_mate(src, dst, k):
        return remote(src, dst, o_send.at[k], o_recv.at[k], dev(g, z, 1 - c, x))

    def half_of(ref, core, size):
        return ref.at[pl.ds(pl.multiple_of(core * size, 16), size), :]

    up_copy = to_mate(half_of(upt, 1 - par, hid), upt_ref, 0)
    dn_copy = to_mate(half_of(dn, 1 - par, hid), dn_ref, 1)
    out_copy = to_mate(outb.at[pl.ds(0, rows), :], out_ref, 2)
    dnt_copy = to_mate(dnt, dnt, 3)
    ht_copy = to_mate(ht, ht, 4)

    part_rows = hid // 2

    def down_part(xs, k):
        first = pl.multiple_of(par * hid + k * part_rows, 16)
        return dn.at[pl.ds(first, part_rows), pl.ds(pl.multiple_of(xs * dcols, 128), dcols)]

    def down_copy(xs, k, d, relayed):
        part = down_part(xs, k)
        return remote(
            part, part, dn_send.at[d, k, relayed], dn_recv.at[d, k, relayed], dev(g, z, par, left if d else right)
        )

    def down_across(xs, k, mine):
        part = dn_part(par if mine else 1 - par, xs)
        return remote(part, part, dy_send.at[k], dy_recv.at[k], dev(other, z, 1 - par, x))

    def piece(xs, k, i):
        cs = par if k == 0 else 1 - par
        return up_rows(nx * i + (2 * nx - 1 - xs + quarter) % nx, cs)

    def x_copy(xs, k, i, slot, to_right):
        d = 0 if to_right else 1
        part = piece(xs, k, i)
        return remote(part, part, x_send.at[d, slot], x_recv.at[d, slot], dev(g, z, par, right if to_right else left))

    def y_copy(i, mine):
        part = piece(x, 0 if mine else 1, i)
        return remote(part, part, y_send.at[i], y_recv.at[i], dev(other, z, 1 - par, x))

    def relay_slot(k, i):
        return 2 * per_col + k * (per_col // 2) + i // 2

    def relay(k, i):

        @pl.when(i % 2 == 0)
        def _():
            x_copy(left, k, i, k * per_col + i, True).wait_recv()
            x_copy(left, k, i, relay_slot(k, i), True).start()

        @pl.when(i % 2 == 1)
        def _():
            x_copy(right, k, i, k * per_col + i, False).wait_recv()
            x_copy(right, k, i, relay_slot(k, i), False).start()

    @pl.when(main)
    def _():
        for k in range(2):
            down_copy(x, k, 0, 0).start()
            down_copy(x, 1 - k, 1, 0).start()
        down_across(x, 0, True).start()

        loads[3].wait()
        block = 64

        def norm(b, carry):
            sl = pl.ds(pl.multiple_of(b * block, block), block)
            values = tok[sl, :].astype(F32)
            center = jnp.mean(values, axis=-1, keepdims=True)
            spread = jnp.mean(jnp.square(values - center), axis=-1, keepdims=True)
            nrm[sl, :] = ((values - center) * lax.rsqrt(spread + 1e-05)).astype(BF16)
            return carry

        lax.fori_loop(0, tok.shape[0] // block, norm, 0)

        down_copy(left, 0, 0, 0).wait_recv()
        down_copy(left, 0, 0, 1).start()
        down_copy(right, 1, 1, 0).wait_recv()
        down_copy(right, 1, 1, 1).start()
        down_copy(left, 1, 0, 0).wait_recv()
        down_across(left, 1, True).start()
        down_copy(right, 0, 1, 0).wait_recv()
        down_across(right, 2, True).start()

        def turn_down(j, carry):
            sl = pl.ds(pl.multiple_of(j * 128, 128), 128)
            dnt[sl, :] = dn[:, sl].T
            return carry

        own_dn = pltpu.make_async_copy(half_of(dn, par, hid), dn_ref, l_sem.at[0])

        def ordered(s):
            away = (s + 1) // 2
            near_first = (z // nx + per_col + jnp.where(s % 2 == 1, away, -away)) % per_col
            return jnp.where(quarter < nx // 2, (s + 1) % per_col, near_first)

        chunk = nx * feat
        acc[...] = jnp.zeros_like(acc)

        def at_lag(s, lag, run):
            @pl.when(jnp.logical_and(s >= lag, s < per_col + lag))
            def _():
                run(ordered(s - lag))

        def arrived(i):
            remote(piece(x, 0, i), piece(x, 0, i), y_send.at[0], zs_recv.at[i], dev(other, z, 1 - par, x)).wait_recv()
            y_copy(i, True).start()
            x_copy(x, 0, i, i, True).start()
            x_copy(x, 0, i, i, False).start()

        def crossed(i):
            y_copy(i, False).wait_recv()
            x_copy(x, 1, i, per_col + i, True).start()
            x_copy(x, 1, i, per_col + i, False).start()

        def complete(i):
            for k in range(2):

                @pl.when(i % 2 == 1)
                def _():
                    x_copy(left, k, i, k * per_col + i, True).wait_recv()
                    x_copy(far, k, i, relay_slot(k, i), False).wait_recv()

                @pl.when(i % 2 == 0)
                def _():
                    x_copy(right, k, i, k * per_col + i, False).wait_recv()
                    x_copy(far, k, i, relay_slot(k, i), True).wait_recv()

            sl = pl.ds(pl.multiple_of(i * chunk, 128), chunk)
            acc[...] += jnp.dot(nrm[:, sl], up[sl, :], preferred_element_type=F32)

        def gather_up(s, carry):
            @pl.when(s == 1)
            def _():
                down_copy(far, 0, 0, 1).wait_recv()
                down_copy(far, 1, 1, 1).wait_recv()
                down_across(far, 3, True).start()

            @pl.when(s == 5)
            def _():
                for k, xs in enumerate((x, left, right, far)):
                    down_across(xs, k, False).wait_recv()
                own_dn.start()
                dn_copy.start()
                lax.fori_loop(0, dn.shape[1] // 128, turn_down, 0)

                @pl.when(apart)
                def _():
                    dnt_copy.start()

            at_lag(s, 0, arrived)
            at_lag(s, 2, crossed)
            at_lag(s, 3, lambda i: relay(0, i))
            at_lag(s, 5, lambda i: relay(1, i))

            at_lag(s, 7, complete)
            return carry

        lax.fori_loop(0, per_col + 7, gather_up, 0)

        ht[...] = jnp.square(jnp.maximum(acc[...], 0.0)).T.astype(BF16)

        @pl.when(apart)
        def _():
            ht_copy.start()

    def turn_up(j, carry):
        sl = pl.ds(pl.multiple_of(j * 128, 128), 128)
        upt[:, sl] = up[sl, :].T
        return carry

    turns = up.shape[0] // 128
    own_up = pltpu.make_async_copy(half_of(upt, par, hid), upt_ref, l_sem.at[1])
    own_out = pltpu.make_async_copy(outb.at[pl.ds(rows, rows), :], out_ref, l_sem.at[2])

    @pl.when(apart)
    def _():
        lax.fori_loop(0, turns, turn_up, 0)
        up_copy.start()
        own_up.start()

    @pl.when(jnp.logical_and(agent, adds))
    def _():
        dnt_copy.wait_recv()
        ht_copy.wait_recv()

    @pl.when(adds)
    def _():
        chains = ((1, 0), (1, 1), (-1, 1), (-1, 0))

        def rs_copy(ch, s, sub, dist):
            sign = chains[ch][0]
            to = (z + nz + sign * dist) % nz
            return remote(
                rs_out.at[ch, s, sub], rs_in.at[ch, s, sub], rs_send.at[ch, s, sub], rs_recv.at[ch, s, sub], dev(g, to, 1, x)
            )

        def rows_of(zt, sub):
            return pl.ds(pl.multiple_of(zt * feat + sub * rows, 16), rows)

        def step(s, skip, first_of):
            for sub in range(2):
                for ch in (1, 2, 0, 3):
                    if ch in skip:
                        continue
                    sign, odd = chains[ch]
                    d = half - odd - 2 * s
                    sl = rows_of((z + 2 * nz + sign * d) % nz, sub)
                    if isinstance(s, int) and s == 0:
                        value = jnp.dot(dnt[sl, :], ht[...], preferred_element_type=F32)
                    else:
                        value = terms[sl, :]
                    if ch not in first_of:
                        rs_copy(ch, s - 1, sub, 2).wait_recv()
                        value = value + rs_in[ch, s - 1, sub].astype(F32)
                    rs_out[ch, s, sub] = value.astype(BF16)
                    rs_copy(ch, s, sub, jnp.minimum(d, 2)).start()

        def turn_some(s):
            @pl.when(main)
            def _():
                lax.fori_loop(4 * s, jnp.minimum(4 * s + 4, turns), turn_up, 0)

        tc = 512

        def all_terms(b, carry):
            sl = pl.ds(pl.multiple_of(b * tc, tc), tc)
            terms[sl, :] = jnp.dot(dnt[sl, :], ht[...], preferred_element_type=F32)
            return carry

        steps = half // 2
        step(0, (3,), (0, 1, 2))
        lax.fori_loop(0, terms.shape[0] // tc, all_terms, 0)
        turn_some(0)
        step(1, (), (3,))
        turn_some(1)

        def steady(s, carry):
            step(s, (), ())

            turn_some(s)
            return carry

        lax.fori_loop(2, steps, steady, 0)
        @pl.when(main)
        def _():
            up_copy.start()
            own_up.start()

        for sub in range(2):
            total = terms[rows_of(z, sub), :]
            for ch in range(4):
                rs_copy(ch, steps - 1, sub, 2).wait_recv()
                total = total + rs_in[ch, steps - 1, sub].astype(F32)
            outb[pl.ds(sub * rows, rows), :] = total.astype(BF16)
        out_copy.start()
        own_out.start()

        def rs_sent(s, carry):
            for sub in range(2):
                for ch in range(3):
                    rs_copy(ch, s, sub, 2).wait_send()

                @pl.when(s > 0)
                def _():
                    rs_copy(3, s, sub, 2).wait_send()

            return carry

        lax.fori_loop(0, steps, rs_sent, 0)
        out_copy.wait_send()
        own_out.wait()

    @pl.when(main)
    def _():
        for k in range(pieces):
            rows_copy(k).wait_send()
        down_copy(left, 0, 0, 1).wait_send()
        down_copy(right, 1, 1, 1).wait_send()
        for d in range(2):
            for k in range(2):
                down_copy(x, k, d, 0).wait_send()
        for k, xs in enumerate((x, left, right, far)):
            down_across(xs, k, True).wait_send()

        def sent(i, carry):
            y_copy(i, True).wait_send()
            for k in range(2):
                x_copy(x, k, i, k * per_col + i, True).wait_send()
                x_copy(x, k, i, k * per_col + i, False).wait_send()

                @pl.when(i % 2 == 0)
                def _():
                    x_copy(left, k, i, relay_slot(k, i), True).wait_send()

                @pl.when(i % 2 == 1)
                def _():
                    x_copy(right, k, i, relay_slot(k, i), False).wait_send()

            return carry

        lax.fori_loop(0, per_col, sent, 0)
        dn_copy.wait_send()
        up_copy.wait_send()
        own_dn = pltpu.make_async_copy(half_of(dn, par, hid), dn_ref, l_sem.at[0])
        own_dn.wait()
        own_up.wait()

    @pl.when(apart)
    def _():
        dnt_copy.wait_send()
        ht_copy.wait_send()

    @pl.when(agent)
    def _():
        loads[3].wait()
        dn_copy.wait_recv()
        up_copy.wait_recv()

    @pl.when(c == 0)
    def _():
        out_copy.wait_recv()

    @pl.when(agent)
    def _():
        def scattered(j, carry):
            scatter_copy(j).wait_send()
            return carry

        lax.fori_loop(0, per_col, scattered, 0)


def result_kernel(*refs):
    sources, results, buffers, (in_sem, out_sem) = refs[:3], refs[3:6], refs[6:9], refs[9:]
    reads, writes = [], []
    for k in range(3):
        size = sources[k].shape[0] // 2 // 16 * 16
        for part, sl in enumerate((pl.ds(0, size), pl.ds(size, sources[k].shape[0] - size))):
            reads.append(pltpu.make_async_copy(sources[k].at[sl], buffers[k].at[sl], in_sem.at[k, part]))
            writes.append(pltpu.make_async_copy(buffers[k].at[sl], results[k].at[sl], out_sem.at[k, part]))
    for read in reads:
        read.start()
    for read, write in zip(reads, writes):
        read.wait()
        write.start()
    for write in writes:
        write.wait()


def solution(mesh):
    nz, nx = mesh.shape["fs"] // 2, mesh.shape["tp"]

    def shards(tokens, up_master, down_master, norm_gain):
        rows = up_master.shape[0]
        hid, dcols = down_master.shape
        count, width = tokens.shape
        feat, wide = 2 * rows, 2 * hid
        steps = nz // 4
        per_col = nz // nx
        dma = pltpu.SemaphoreType.DMA
        any_space = pl.BlockSpec(memory_space=pltpu.HBM)
        results = pl.pallas_call(
            functools.partial(kernel, nz, nx),
            out_shape=(
                jax.ShapeDtypeStruct((rows, count), BF16),
                jax.ShapeDtypeStruct((hid, width), BF16),
                jax.ShapeDtypeStruct((hid, width), BF16),
            ),
            in_specs=[any_space] * 4,
            out_specs=(any_space,) * 3,
            scratch_shapes=[
                pltpu.VMEM((count, width), BF16),
                pltpu.VMEM(up_master.shape, F32),
                pltpu.VMEM(down_master.shape, F32),
                pltpu.VMEM((1, rows), F32),
                pltpu.VMEM(up_master.shape, BF16),
                pltpu.VMEM(up_master.shape, BF16),
                pltpu.VMEM((width, wide), BF16),
                pltpu.VMEM((wide, width), BF16),
                pltpu.VMEM((count, width), BF16),
                pltpu.VMEM((width, wide), BF16),
                pltpu.VMEM((wide, width), BF16),
                pltpu.VMEM((count, wide), F32),
                pltpu.VMEM((wide, count), BF16),
                pltpu.VMEM((width, count), F32),
                pltpu.VMEM((4, steps, 2, rows, count), BF16),
                pltpu.VMEM((4, steps, 2, rows, count), BF16),
                pltpu.VMEM((feat, count), BF16),
                dma((4,)),
                dma((4,)),
                dma((4,)),
                dma((4,)),
                dma((4,)),
                dma((per_col,)),
                dma((per_col,)),
                dma((per_col,)),
                dma((per_col,)),
                dma((2, 3 * per_col)),
                dma((2, 3 * per_col)),
                dma((2, 2, 2)),
                dma((2, 2, 2)),
                dma((4, steps, 2)),
                dma((4, steps, 2)),
                dma((5,)),
                dma((5,)),
                dma((3,)),
            ],
            compiler_params=pltpu.CompilerParams(
                collective_id=0, has_side_effects=True, vmem_limit_bytes=60 * 1024 * 1024
            ),
        )(tokens, up_master, down_master, norm_gain[None])
        out_t, up_t, down = pl.pallas_call(
            result_kernel,
            out_shape=tuple(jax.ShapeDtypeStruct(r.shape, r.dtype) for r in results),
            in_specs=[any_space] * 3,
            out_specs=(any_space,) * 3,
            scratch_shapes=[pltpu.VMEM(r.shape, r.dtype) for r in results] + [dma((3, 2)), dma((3, 2))],
            compiler_params=pltpu.CompilerParams(vmem_limit_bytes=60 * 1024 * 1024),
        )(*results)
        return out_t.T, up_t.T, down

    return jax.shard_map(
        shards,
        mesh=mesh,
        in_specs=(P(("grp", "tp"), None), P("fs", "tp"), P("fs", "tp"), P("fs")),
        out_specs=(P(("grp", "tp"), "fs"), P("grp", "fs"), P(("grp", "fs"), None)),
        check_vma=False,
    )
```

```python
import functools

import jax
import jax.numpy as jnp
from jax import lax
from jax.experimental import pallas as pl
from jax.experimental.pallas import tpu as pltpu
from jax.sharding import PartitionSpec as P

MESH = pl.DeviceIdType.MESH
BF16 = jnp.bfloat16
F32 = jnp.float32


def kernel(
    nz, nx, tok_hbm, upm_hbm, dnm_hbm, gain_hbm, out_ref, upt_ref, dn_ref,
    tok, upm, dnm, gain, stage, slots, up, dn, nrm, dnt, upt, acc, ht, terms, rs_out, rs_in, outb,
    in_sem, xa_send, xa_recv, dy_send, dy_recv, zs_send, zs_recv, y_send, y_recv, x_send, x_recv, dn_send, dn_recv,
    rs_send, rs_recv, o_send, o_recv, l_sem,
):
    g, fs, x = lax.axis_index("grp"), lax.axis_index("fs"), lax.axis_index("tp")
    z, c = fs // 2, fs % 2
    par = g % 2
    other = g + 1 - 2 * par
    main = c == par
    agent = c != par
    adds = c == 1
    apart = jnp.logical_and(main, c == 0)
    right, left = (x + 1) % nx, (x + nx - 1) % nx
    per_col = nz // nx
    quarter = z // per_col
    shift = (nx - 1) - z % nx
    served = (x + nx - shift) % nx
    residue = (2 * nx - 1 - x + quarter) % nx
    far = (x + 2) % nx
    half = nz // 2
    rows = upm.shape[0]
    hid = dnm.shape[0]
    dcols = dnm.shape[1]
    wide = 2 * hid
    feat = 2 * rows

    def dev(g_, z_, c_, x_):
        return {"grp": g_, "fs": 2 * z_ + c_, "tp": x_}

    def remote(src, dst, ssem, rsem, to):
        return pltpu.make_async_remote_copy(
            src_ref=src, dst_ref=dst, send_sem=ssem, recv_sem=rsem, device_id=to, device_id_type=MESH
        )

    def up_rows(zs, cs):
        return up.at[pl.ds(pl.multiple_of((2 * zs + cs) * rows, 16), rows), :]

    def dn_part(h, xs):
        return dn.at[pl.ds(h * hid, hid), pl.ds(pl.multiple_of(xs * dcols, 128), dcols)]

    loads = [
        pltpu.make_async_copy(upm_hbm, upm, in_sem.at[0]),
        pltpu.make_async_copy(gain_hbm, gain, in_sem.at[1]),
        pltpu.make_async_copy(dnm_hbm, dnm, in_sem.at[2]),
        pltpu.make_async_copy(tok_hbm, tok, in_sem.at[3]),
    ]
    for k in range(4):
        loads[k].start()

    barrier = pltpu.get_barrier_semaphore()

    def greet(to):
        pl.semaphore_signal(barrier, inc=1, device_id=to, device_id_type=MESH)

    @pl.when(main)
    def _():
        def greet_agent(i, carry):
            greet(dev(g, i * nx + residue, 1 - par, x))
            return carry

        lax.fori_loop(0, per_col, greet_agent, 0)
        for to_x in (right, left):
            greet(dev(g, z, par, to_x))
        greet(dev(g, z, 1 - par, x))
        greet(dev(other, z, 1 - par, x))

    @pl.when(agent)
    def _():
        greet(dev(g, z, par, x))
        greet(dev(g, z, par, served))

    @pl.when(adds)
    def _():
        for d in (1, 2, nz - 1, nz - 2):
            greet(dev(g, (z + d) % nz, 1, x))

    loads[0].wait()
    loads[1].wait()

    @pl.when(main)
    def _():
        eye = lax.broadcasted_iota(jnp.int32, (rows, rows), 0) == lax.broadcasted_iota(jnp.int32, (rows, rows), 1)
        scale = jnp.sum(jnp.where(eye, gain[...], 0.0), axis=1, keepdims=True)
        stage[...] = (scale * upm[...]).astype(BF16)

    loads[2].wait()

    @pl.when(main)
    def _():
        dn_part(par, x)[...] = dnm[...].astype(BF16)

    peers = jnp.where(main, 5, 1 + per_col) + jnp.where(adds, 4, 0)
    pl.semaphore_wait(barrier, peers)

    pieces = 4
    per_piece = per_col // pieces

    def rows_copy(k):
        sl = pl.ds(k * per_piece * wide, per_piece * wide)
        return remote(
            stage.at[:, sl], slots.at[:, sl], xa_send.at[k], xa_recv.at[k], dev(g, z, 1 - par, (x + shift) % nx)
        )

    @pl.when(main)
    def _():
        for k in range(pieces):
            rows_copy(k).start()

    def scatter_copy(j):
        part = slots.at[:, pl.ds(pl.multiple_of(j * wide, 128), wide)]
        return remote(
            part, up_rows(z, par), zs_send.at[j], zs_recv.at[z // nx], dev(g, per_col * served + j, par, x)
        )

    @pl.when(agent)
    def _():
        for k in range(pieces):
            rows_copy(k).wait_recv()
            for j in range(per_piece):
                scatter_copy(k * per_piece + j).start()

    def to_mate(src, dst, k):
        return remote(src, dst, o_send.at[k], o_recv.at[k], dev(g, z, 1 - c, x))

    def half_of(ref, core, size):
        return ref.at[pl.ds(pl.multiple_of(core * size, 16), size), :]

    up_copy = to_mate(half_of(upt, 1 - par, hid), upt_ref, 0)
    dn_copy = to_mate(half_of(dn, 1 - par, hid), dn_ref, 1)
    out_copy = to_mate(outb.at[pl.ds(0, rows), :], out_ref, 2)
    dnt_copy = to_mate(dnt, dnt, 3)
    ht_copy = to_mate(ht, ht, 4)

    part_rows = hid // 2

    def down_part(xs, k):
        first = pl.multiple_of(par * hid + k * part_rows, 16)
        return dn.at[pl.ds(first, part_rows), pl.ds(pl.multiple_of(xs * dcols, 128), dcols)]

    def down_copy(xs, k, d, relayed):
        part = down_part(xs, k)
        return remote(
            part, part, dn_send.at[d, k, relayed], dn_recv.at[d, k, relayed], dev(g, z, par, left if d else right)
        )

    def down_across(xs, k, mine):
        part = dn_part(par if mine else 1 - par, xs)
        return remote(part, part, dy_send.at[k], dy_recv.at[k], dev(other, z, 1 - par, x))

    def piece(xs, k, i):
        cs = par if k == 0 else 1 - par
        return up_rows(nx * i + (2 * nx - 1 - xs + quarter) % nx, cs)

    def x_copy(xs, k, i, slot, to_right):
        d = 0 if to_right else 1
        part = piece(xs, k, i)
        return remote(part, part, x_send.at[d, slot], x_recv.at[d, slot], dev(g, z, par, right if to_right else left))

    def y_copy(i, mine):
        part = piece(x, 0 if mine else 1, i)
        return remote(part, part, y_send.at[i], y_recv.at[i], dev(other, z, 1 - par, x))

    def relay_slot(k, i):
        return 2 * per_col + k * (per_col // 2) + i // 2

    def relay(k, i):

        @pl.when(i % 2 == 0)
        def _():
            x_copy(left, k, i, k * per_col + i, True).wait_recv()
            x_copy(left, k, i, relay_slot(k, i), True).start()

        @pl.when(i % 2 == 1)
        def _():
            x_copy(right, k, i, k * per_col + i, False).wait_recv()
            x_copy(right, k, i, relay_slot(k, i), False).start()

    @pl.when(main)
    def _():
        for k in range(2):
            down_copy(x, k, 0, 0).start()
            down_copy(x, 1 - k, 1, 0).start()
        down_across(x, 0, True).start()

        loads[3].wait()
        block = 64

        def norm(b, carry):
            sl = pl.ds(pl.multiple_of(b * block, block), block)
            values = tok[sl, :].astype(F32)
            center = jnp.mean(values, axis=-1, keepdims=True)
            spread = jnp.mean(jnp.square(values - center), axis=-1, keepdims=True)
            nrm[sl, :] = ((values - center) * lax.rsqrt(spread + 1e-05)).astype(BF16)
            return carry

        lax.fori_loop(0, tok.shape[0] // block, norm, 0)

        down_copy(left, 0, 0, 0).wait_recv()
        down_copy(left, 0, 0, 1).start()
        down_copy(right, 1, 1, 0).wait_recv()
        down_copy(right, 1, 1, 1).start()
        down_copy(left, 1, 0, 0).wait_recv()
        down_across(left, 1, True).start()
        down_copy(right, 0, 1, 0).wait_recv()
        down_across(right, 2, True).start()

        def turn_down(j, carry):
            sl = pl.ds(pl.multiple_of(j * 128, 128), 128)
            dnt[sl, :] = dn[:, sl].T
            return carry

        own_dn = pltpu.make_async_copy(half_of(dn, par, hid), dn_ref, l_sem.at[0])

        def ordered(s):
            away = (s + 1) // 2
            near_first = (z // nx + per_col + jnp.where(s % 2 == 1, away, -away)) % per_col
            return jnp.where(quarter < nx // 2, (s + 1) % per_col, near_first)

        chunk = nx * feat
        acc[...] = jnp.zeros_like(acc)

        def at_lag(s, lag, run):
            @pl.when(jnp.logical_and(s >= lag, s < per_col + lag))
            def _():
                run(ordered(s - lag))

        def arrived(i):
            remote(piece(x, 0, i), piece(x, 0, i), y_send.at[0], zs_recv.at[i], dev(other, z, 1 - par, x)).wait_recv()
            y_copy(i, True).start()
            x_copy(x, 0, i, i, True).start()
            x_copy(x, 0, i, i, False).start()

        def crossed(i):
            y_copy(i, False).wait_recv()
            x_copy(x, 1, i, per_col + i, True).start()
            x_copy(x, 1, i, per_col + i, False).start()

        def complete(i):
            for k in range(2):

                @pl.when(i % 2 == 1)
                def _():
                    x_copy(left, k, i, k * per_col + i, True).wait_recv()
                    x_copy(far, k, i, relay_slot(k, i), False).wait_recv()

                @pl.when(i % 2 == 0)
                def _():
                    x_copy(right, k, i, k * per_col + i, False).wait_recv()
                    x_copy(far, k, i, relay_slot(k, i), True).wait_recv()

            sl = pl.ds(pl.multiple_of(i * chunk, 128), chunk)
            acc[...] += jnp.dot(nrm[:, sl], up[sl, :], preferred_element_type=F32)

        def gather_up(s, carry):
            @pl.when(s == 1)
            def _():
                down_copy(far, 0, 0, 1).wait_recv()
                down_copy(far, 1, 1, 1).wait_recv()
                down_across(far, 3, True).start()

            @pl.when(s == 5)
            def _():
                for k, xs in enumerate((x, left, right, far)):
                    down_across(xs, k, False).wait_recv()
                own_dn.start()
                dn_copy.start()
                lax.fori_loop(0, dn.shape[1] // 128, turn_down, 0)

                @pl.when(apart)
                def _():
                    dnt_copy.start()

            at_lag(s, 0, arrived)
            at_lag(s, 2, crossed)
            at_lag(s, 3, lambda i: relay(0, i))
            at_lag(s, 5, lambda i: relay(1, i))

            at_lag(s, 7, complete)
            return carry

        lax.fori_loop(0, per_col + 7, gather_up, 0)

        ht[...] = jnp.square(jnp.maximum(acc[...], 0.0)).T.astype(BF16)

        @pl.when(apart)
        def _():
            ht_copy.start()

    def turn_up(j, carry):
        sl = pl.ds(pl.multiple_of(j * 128, 128), 128)
        upt[:, sl] = up[sl, :].T
        return carry

    turns = up.shape[0] // 128
    own_up = pltpu.make_async_copy(half_of(upt, par, hid), upt_ref, l_sem.at[1])
    own_out = pltpu.make_async_copy(outb.at[pl.ds(rows, rows), :], out_ref, l_sem.at[2])

    @pl.when(apart)
    def _():
        lax.fori_loop(0, turns, turn_up, 0)
        up_copy.start()
        own_up.start()

    @pl.when(jnp.logical_and(agent, adds))
    def _():
        dnt_copy.wait_recv()
        ht_copy.wait_recv()

    @pl.when(adds)
    def _():
        chains = ((1, 0), (1, 1), (-1, 1), (-1, 0))

        def rs_copy(ch, s, sub, dist):
            sign = chains[ch][0]
            to = (z + nz + sign * dist) % nz
            return remote(
                rs_out.at[ch, s, sub], rs_in.at[ch, s, sub], rs_send.at[ch, s, sub], rs_recv.at[ch, s, sub], dev(g, to, 1, x)
            )

        def rows_of(zt, sub):
            return pl.ds(pl.multiple_of(zt * feat + sub * rows, 16), rows)

        def step(s, runs, first_of):
            for pair in ((1, 2), (0, 3)):
                for sub, ch in ((0, pair[0]), (0, pair[1]), (1, pair[0]), (1, pair[1])):
                    if ch not in runs:
                        continue
                    sign, odd = chains[ch]
                    d = half - odd - 2 * s
                    sl = rows_of((z + 2 * nz + sign * d) % nz, sub)
                    if isinstance(s, int) and s == 0:
                        value = jnp.dot(dnt[sl, :], ht[...], preferred_element_type=F32)
                    else:
                        value = terms[sl, :]
                    if ch not in first_of:
                        rs_copy(ch, s - 1, sub, 2).wait_recv()
                        value = value + rs_in[ch, s - 1, sub].astype(F32)
                    rs_out[ch, s, sub] = value.astype(BF16)
                    rs_copy(ch, s, sub, jnp.minimum(d, 2)).start()

        def turn_some(s):
            @pl.when(main)
            def _():
                lax.fori_loop(4 * s, jnp.minimum(4 * s + 4, turns), turn_up, 0)

        tc = 512

        def all_terms(b, carry):
            sl = pl.ds(pl.multiple_of(b * tc, tc), tc)
            terms[sl, :] = jnp.dot(dnt[sl, :], ht[...], preferred_element_type=F32)
            return carry

        steps = half // 2
        step(0, (1, 2), (1, 2))
        lax.fori_loop(0, terms.shape[0] // tc, all_terms, 0)
        step(0, (0,), (0,))
        turn_some(0)
        step(1, (0, 1, 2, 3), (3,))
        turn_some(1)

        def steady(s, carry):
            step(s, (0, 1, 2, 3), ())

            turn_some(s)
            return carry

        lax.fori_loop(2, steps, steady, 0)
        @pl.when(main)
        def _():
            up_copy.start()
            own_up.start()

        for sub in range(2):
            total = terms[rows_of(z, sub), :]
            for ch in range(4):
                rs_copy(ch, steps - 1, sub, 2).wait_recv()
                total = total + rs_in[ch, steps - 1, sub].astype(F32)
            outb[pl.ds(sub * rows, rows), :] = total.astype(BF16)
        out_copy.start()
        own_out.start()

        def rs_sent(s, carry):
            for sub in range(2):
                for ch in range(3):
                    rs_copy(ch, s, sub, 2).wait_send()

                @pl.when(s > 0)
                def _():
                    rs_copy(3, s, sub, 2).wait_send()

            return carry

        lax.fori_loop(0, steps, rs_sent, 0)
        out_copy.wait_send()
        own_out.wait()

    @pl.when(main)
    def _():
        for k in range(pieces):
            rows_copy(k).wait_send()
        down_copy(left, 0, 0, 1).wait_send()
        down_copy(right, 1, 1, 1).wait_send()
        for d in range(2):
            for k in range(2):
                down_copy(x, k, d, 0).wait_send()
        for k, xs in enumerate((x, left, right, far)):
            down_across(xs, k, True).wait_send()

        def sent(i, carry):
            y_copy(i, True).wait_send()
            for k in range(2):
                x_copy(x, k, i, k * per_col + i, True).wait_send()
                x_copy(x, k, i, k * per_col + i, False).wait_send()

                @pl.when(i % 2 == 0)
                def _():
                    x_copy(left, k, i, relay_slot(k, i), True).wait_send()

                @pl.when(i % 2 == 1)
                def _():
                    x_copy(right, k, i, relay_slot(k, i), False).wait_send()

            return carry

        lax.fori_loop(0, per_col, sent, 0)
        dn_copy.wait_send()
        up_copy.wait_send()
        own_dn = pltpu.make_async_copy(half_of(dn, par, hid), dn_ref, l_sem.at[0])
        own_dn.wait()
        own_up.wait()

    @pl.when(apart)
    def _():
        dnt_copy.wait_send()
        ht_copy.wait_send()

    @pl.when(agent)
    def _():
        loads[3].wait()
        dn_copy.wait_recv()
        up_copy.wait_recv()

    @pl.when(c == 0)
    def _():
        out_copy.wait_recv()

    @pl.when(agent)
    def _():
        def scattered(j, carry):
            scatter_copy(j).wait_send()
            return carry

        lax.fori_loop(0, per_col, scattered, 0)


def result_kernel(*refs):
    sources, results, buffers, (in_sem, out_sem) = refs[:3], refs[3:6], refs[6:9], refs[9:]
    reads, writes = [], []
    for k in range(3):
        size = sources[k].shape[0] // 2 // 16 * 16
        for part, sl in enumerate((pl.ds(0, size), pl.ds(size, sources[k].shape[0] - size))):
            reads.append(pltpu.make_async_copy(sources[k].at[sl], buffers[k].at[sl], in_sem.at[k, part]))
            writes.append(pltpu.make_async_copy(buffers[k].at[sl], results[k].at[sl], out_sem.at[k, part]))
    for read in reads:
        read.start()
    for read, write in zip(reads, writes):
        read.wait()
        write.start()
    for write in writes:
        write.wait()


def solution(mesh):
    nz, nx = mesh.shape["fs"] // 2, mesh.shape["tp"]

    def shards(tokens, up_master, down_master, norm_gain):
        rows = up_master.shape[0]
        hid, dcols = down_master.shape
        count, width = tokens.shape
        feat, wide = 2 * rows, 2 * hid
        steps = nz // 4
        per_col = nz // nx
        dma = pltpu.SemaphoreType.DMA
        any_space = pl.BlockSpec(memory_space=pltpu.HBM)
        results = pl.pallas_call(
            functools.partial(kernel, nz, nx),
            out_shape=(
                jax.ShapeDtypeStruct((rows, count), BF16),
                jax.ShapeDtypeStruct((hid, width), BF16),
                jax.ShapeDtypeStruct((hid, width), BF16),
            ),
            in_specs=[any_space] * 4,
            out_specs=(any_space,) * 3,
            scratch_shapes=[
                pltpu.VMEM((count, width), BF16),
                pltpu.VMEM(up_master.shape, F32),
                pltpu.VMEM(down_master.shape, F32),
                pltpu.VMEM((1, rows), F32),
                pltpu.VMEM(up_master.shape, BF16),
                pltpu.VMEM(up_master.shape, BF16),
                pltpu.VMEM((width, wide), BF16),
                pltpu.VMEM((wide, width), BF16),
                pltpu.VMEM((count, width), BF16),
                pltpu.VMEM((width, wide), BF16),
                pltpu.VMEM((wide, width), BF16),
                pltpu.VMEM((count, wide), F32),
                pltpu.VMEM((wide, count), BF16),
                pltpu.VMEM((width, count), F32),
                pltpu.VMEM((4, steps, 2, rows, count), BF16),
                pltpu.VMEM((4, steps, 2, rows, count), BF16),
                pltpu.VMEM((feat, count), BF16),
                dma((4,)),
                dma((4,)),
                dma((4,)),
                dma((4,)),
                dma((4,)),
                dma((per_col,)),
                dma((per_col,)),
                dma((per_col,)),
                dma((per_col,)),
                dma((2, 3 * per_col)),
                dma((2, 3 * per_col)),
                dma((2, 2, 2)),
                dma((2, 2, 2)),
                dma((4, steps, 2)),
                dma((4, steps, 2)),
                dma((5,)),
                dma((5,)),
                dma((3,)),
            ],
            compiler_params=pltpu.CompilerParams(
                collective_id=0, has_side_effects=True, vmem_limit_bytes=60 * 1024 * 1024
            ),
        )(tokens, up_master, down_master, norm_gain[None])
        out_t, up_t, down = pl.pallas_call(
            result_kernel,
            out_shape=tuple(jax.ShapeDtypeStruct(r.shape, r.dtype) for r in results),
            in_specs=[any_space] * 3,
            out_specs=(any_space,) * 3,
            scratch_shapes=[pltpu.VMEM(r.shape, r.dtype) for r in results] + [dma((3, 2)), dma((3, 2))],
            compiler_params=pltpu.CompilerParams(vmem_limit_bytes=60 * 1024 * 1024),
        )(*results)
        return out_t.T, up_t.T, down

    return jax.shard_map(
        shards,
        mesh=mesh,
        in_specs=(P(("grp", "tp"), None), P("fs", "tp"), P("fs", "tp"), P("fs")),
        out_specs=(P(("grp", "tp"), "fs"), P("grp", "fs"), P(("grp", "fs"), None)),
        check_vma=False,
    )
```

```python
import functools

import jax
import jax.numpy as jnp
from jax import lax
from jax.experimental import pallas as pl
from jax.experimental.pallas import tpu as pltpu
from jax.sharding import PartitionSpec as P

MESH = pl.DeviceIdType.MESH
BF16 = jnp.bfloat16
F32 = jnp.float32


def kernel(
    nz, nx, tok_hbm, upm_hbm, dnm_hbm, gain_hbm, out_ref, upt_ref, dn_ref,
    tok, upm, dnm, gain, stage, slots, up, dn, nrm, dnt, upt, acc, ht, terms, rs_out, rs_in, outb,
    in_sem, xa_send, xa_recv, dy_send, dy_recv, zs_send, zs_recv, y_send, y_recv, x_send, x_recv, dn_send, dn_recv,
    rs_send, rs_recv, o_send, o_recv, l_sem,
):
    g, fs, x = lax.axis_index("grp"), lax.axis_index("fs"), lax.axis_index("tp")
    z, c = fs // 2, fs % 2
    par = g % 2
    other = g + 1 - 2 * par
    main = c == par
    agent = c != par
    adds = c == 1
    apart = jnp.logical_and(main, c == 0)
    right, left = (x + 1) % nx, (x + nx - 1) % nx
    per_col = nz // nx
    quarter = z // per_col
    shift = (nx - 1) - z % nx
    served = (x + nx - shift) % nx
    residue = (2 * nx - 1 - x + quarter) % nx
    far = (x + 2) % nx
    half = nz // 2
    rows = upm.shape[0]
    hid = dnm.shape[0]
    dcols = dnm.shape[1]
    wide = 2 * hid
    feat = 2 * rows

    def dev(g_, z_, c_, x_):
        return {"grp": g_, "fs": 2 * z_ + c_, "tp": x_}

    def remote(src, dst, ssem, rsem, to):
        return pltpu.make_async_remote_copy(
            src_ref=src, dst_ref=dst, send_sem=ssem, recv_sem=rsem, device_id=to, device_id_type=MESH
        )

    def up_rows(zs, cs):
        return up.at[pl.ds(pl.multiple_of((2 * zs + cs) * rows, 16), rows), :]

    def dn_part(h, xs):
        return dn.at[pl.ds(h * hid, hid), pl.ds(pl.multiple_of(xs * dcols, 128), dcols)]

    loads = [
        pltpu.make_async_copy(upm_hbm, upm, in_sem.at[0]),
        pltpu.make_async_copy(gain_hbm, gain, in_sem.at[1]),
        pltpu.make_async_copy(dnm_hbm, dnm, in_sem.at[2]),
        pltpu.make_async_copy(tok_hbm, tok, in_sem.at[3]),
    ]
    for k in range(4):
        loads[k].start()

    barrier = pltpu.get_barrier_semaphore()

    def greet(to):
        pl.semaphore_signal(barrier, inc=1, device_id=to, device_id_type=MESH)

    @pl.when(main)
    def _():
        def greet_agent(i, carry):
            greet(dev(g, i * nx + residue, 1 - par, x))
            return carry

        lax.fori_loop(0, per_col, greet_agent, 0)
        for to_x in (right, left):
            greet(dev(g, z, par, to_x))
        greet(dev(g, z, 1 - par, x))
        greet(dev(other, z, 1 - par, x))

    @pl.when(agent)
    def _():
        greet(dev(g, z, par, x))
        greet(dev(g, z, par, served))

    @pl.when(adds)
    def _():
        for d in (1, 2, nz - 1, nz - 2):
            greet(dev(g, (z + d) % nz, 1, x))

    loads[0].wait()
    loads[1].wait()

    @pl.when(main)
    def _():
        eye = lax.broadcasted_iota(jnp.int32, (rows, rows), 0) == lax.broadcasted_iota(jnp.int32, (rows, rows), 1)
        scale = jnp.sum(jnp.where(eye, gain[...], 0.0), axis=1, keepdims=True)
        stage[...] = (scale * upm[...]).astype(BF16)

    loads[2].wait()

    @pl.when(main)
    def _():
        dn_part(par, x)[...] = dnm[...].astype(BF16)

    peers = jnp.where(main, 5, 1 + per_col) + jnp.where(adds, 4, 0)
    pl.semaphore_wait(barrier, peers)

    pieces = 4
    per_piece = per_col // pieces

    def rows_copy(k):
        sl = pl.ds(k * per_piece * wide, per_piece * wide)
        return remote(
            stage.at[:, sl], slots.at[:, sl], xa_send.at[k], xa_recv.at[k], dev(g, z, 1 - par, (x + shift) % nx)
        )

    @pl.when(main)
    def _():
        for k in range(pieces):
            rows_copy(k).start()

    def scatter_copy(j):
        part = slots.at[:, pl.ds(pl.multiple_of(j * wide, 128), wide)]
        return remote(
            part, up_rows(z, par), zs_send.at[j], zs_recv.at[z // nx], dev(g, per_col * served + j, par, x)
        )

    @pl.when(agent)
    def _():
        for k in range(pieces):
            rows_copy(k).wait_recv()
            for j in range(per_piece):
                scatter_copy(k * per_piece + j).start()

    def to_mate(src, dst, k):
        return remote(src, dst, o_send.at[k], o_recv.at[k], dev(g, z, 1 - c, x))

    def half_of(ref, core, size):
        return ref.at[pl.ds(pl.multiple_of(core * size, 16), size), :]

    up_copy = to_mate(half_of(upt, 1 - par, hid), upt_ref, 0)
    dn_copy = to_mate(half_of(dn, 1 - par, hid), dn_ref, 1)
    out_copy = to_mate(outb.at[pl.ds(0, rows), :], out_ref, 2)
    dnt_copy = to_mate(dnt, dnt, 3)
    ht_copy = to_mate(ht, ht, 4)

    part_rows = hid // 2

    def down_part(xs, k):
        first = pl.multiple_of(par * hid + k * part_rows, 16)
        return dn.at[pl.ds(first, part_rows), pl.ds(pl.multiple_of(xs * dcols, 128), dcols)]

    def down_copy(xs, k, d, relayed):
        part = down_part(xs, k)
        return remote(
            part, part, dn_send.at[d, k, relayed], dn_recv.at[d, k, relayed], dev(g, z, par, left if d else right)
        )

    def down_across(xs, k, mine):
        part = dn_part(par if mine else 1 - par, xs)
        return remote(part, part, dy_send.at[k], dy_recv.at[k], dev(other, z, 1 - par, x))

    def piece(xs, k, i):
        cs = par if k == 0 else 1 - par
        return up_rows(nx * i + (2 * nx - 1 - xs + quarter) % nx, cs)

    def x_copy(xs, k, i, slot, to_right):
        d = 0 if to_right else 1
        part = piece(xs, k, i)
        return remote(part, part, x_send.at[d, slot], x_recv.at[d, slot], dev(g, z, par, right if to_right else left))

    def y_copy(i, mine):
        part = piece(x, 0 if mine else 1, i)
        return remote(part, part, y_send.at[i], y_recv.at[i], dev(other, z, 1 - par, x))

    def relay_slot(k, i):
        return 2 * per_col + k * (per_col // 2) + i // 2

    def relay(k, i):

        @pl.when(i % 2 == 0)
        def _():
            x_copy(left, k, i, k * per_col + i, True).wait_recv()
            x_copy(left, k, i, relay_slot(k, i), True).start()

        @pl.when(i % 2 == 1)
        def _():
            x_copy(right, k, i, k * per_col + i, False).wait_recv()
            x_copy(right, k, i, relay_slot(k, i), False).start()

    @pl.when(main)
    def _():
        for k in range(2):
            down_copy(x, k, 0, 0).start()
            down_copy(x, 1 - k, 1, 0).start()
        down_across(x, 0, True).start()

        loads[3].wait()
        block = 64

        def norm(b, carry):
            sl = pl.ds(pl.multiple_of(b * block, block), block)
            values = tok[sl, :].astype(F32)
            center = jnp.mean(values, axis=-1, keepdims=True)
            spread = jnp.mean(jnp.square(values - center), axis=-1, keepdims=True)
            nrm[sl, :] = ((values - center) * lax.rsqrt(spread + 1e-05)).astype(BF16)
            return carry

        lax.fori_loop(0, tok.shape[0] // block, norm, 0)

        down_copy(left, 0, 0, 0).wait_recv()
        down_copy(left, 0, 0, 1).start()
        down_copy(right, 1, 1, 0).wait_recv()
        down_copy(right, 1, 1, 1).start()
        down_copy(left, 1, 0, 0).wait_recv()
        down_across(left, 1, True).start()
        down_copy(right, 0, 1, 0).wait_recv()
        down_across(right, 2, True).start()

        def turn_down(j, carry):
            sl = pl.ds(pl.multiple_of(j * 128, 128), 128)
            dnt[sl, :] = dn[:, sl].T
            return carry

        own_dn = pltpu.make_async_copy(half_of(dn, par, hid), dn_ref, l_sem.at[0])

        def ordered(s):
            away = (s + 1) // 2
            near_first = (z // nx + per_col + jnp.where(s % 2 == 1, away, -away)) % per_col
            falling = (2 * per_col - 2 - s) % per_col
            return jnp.where(quarter < nx // 2, (s + 1) % per_col, jnp.where(quarter < nx - 1, falling, near_first))

        chunk = nx * feat
        acc[...] = jnp.zeros_like(acc)

        def at_lag(s, lag, run):
            @pl.when(jnp.logical_and(s >= lag, s < per_col + lag))
            def _():
                run(ordered(s - lag))

        def arrived(i):
            remote(piece(x, 0, i), piece(x, 0, i), y_send.at[0], zs_recv.at[i], dev(other, z, 1 - par, x)).wait_recv()
            y_copy(i, True).start()
            x_copy(x, 0, i, i, True).start()
            x_copy(x, 0, i, i, False).start()

        def crossed(i):
            y_copy(i, False).wait_recv()
            x_copy(x, 1, i, per_col + i, True).start()
            x_copy(x, 1, i, per_col + i, False).start()

        def complete(i):
            for k in range(2):

                @pl.when(i % 2 == 1)
                def _():
                    x_copy(left, k, i, k * per_col + i, True).wait_recv()
                    x_copy(far, k, i, relay_slot(k, i), False).wait_recv()

                @pl.when(i % 2 == 0)
                def _():
                    x_copy(right, k, i, k * per_col + i, False).wait_recv()
                    x_copy(far, k, i, relay_slot(k, i), True).wait_recv()

            sl = pl.ds(pl.multiple_of(i * chunk, 128), chunk)
            acc[...] += jnp.dot(nrm[:, sl], up[sl, :], preferred_element_type=F32)

        def gather_up(s, carry):
            @pl.when(s == 1)
            def _():
                down_copy(far, 0, 0, 1).wait_recv()
                down_copy(far, 1, 1, 1).wait_recv()
                down_across(far, 3, True).start()

            @pl.when(s == 5)
            def _():
                for k, xs in enumerate((x, left, right, far)):
                    down_across(xs, k, False).wait_recv()
                own_dn.start()
                dn_copy.start()
                lax.fori_loop(0, dn.shape[1] // 128, turn_down, 0)

                @pl.when(apart)
                def _():
                    dnt_copy.start()

            at_lag(s, 0, arrived)
            at_lag(s, 2, crossed)
            at_lag(s, 3, lambda i: relay(0, i))
            at_lag(s, 5, lambda i: relay(1, i))

            at_lag(s, 7, complete)
            return carry

        lax.fori_loop(0, per_col + 7, gather_up, 0)

        ht[...] = jnp.square(jnp.maximum(acc[...], 0.0)).T.astype(BF16)

        @pl.when(apart)
        def _():
            ht_copy.start()

    def turn_up(j, carry):
        sl = pl.ds(pl.multiple_of(j * 128, 128), 128)
        upt[:, sl] = up[sl, :].T
        return carry

    turns = up.shape[0] // 128
    own_up = pltpu.make_async_copy(half_of(upt, par, hid), upt_ref, l_sem.at[1])
    own_out = pltpu.make_async_copy(outb.at[pl.ds(rows, rows), :], out_ref, l_sem.at[2])

    @pl.when(apart)
    def _():
        lax.fori_loop(0, turns, turn_up, 0)
        up_copy.start()
        own_up.start()

    @pl.when(jnp.logical_and(agent, adds))
    def _():
        dnt_copy.wait_recv()
        ht_copy.wait_recv()

    @pl.when(adds)
    def _():
        chains = ((1, 0), (1, 1), (-1, 1), (-1, 0))

        def rs_copy(ch, s, sub, dist):
            sign = chains[ch][0]
            to = (z + nz + sign * dist) % nz
            return remote(
                rs_out.at[ch, s, sub], rs_in.at[ch, s, sub], rs_send.at[ch, s, sub], rs_recv.at[ch, s, sub], dev(g, to, 1, x)
            )

        def rows_of(zt, sub):
            return pl.ds(pl.multiple_of(zt * feat + sub * rows, 16), rows)

        def step(s, skip, first_of):
            for sub in range(2):
                for ch in (1, 2, 0, 3):
                    if ch in skip:
                        continue
                    sign, odd = chains[ch]
                    d = half - odd - 2 * s
                    sl = rows_of((z + 2 * nz + sign * d) % nz, sub)
                    if isinstance(s, int) and s == 0:
                        value = jnp.dot(dnt[sl, :], ht[...], preferred_element_type=F32)
                    else:
                        value = terms[sl, :]
                    if ch not in first_of:
                        rs_copy(ch, s - 1, sub, 2).wait_recv()
                        value = value + rs_in[ch, s - 1, sub].astype(F32)
                    rs_out[ch, s, sub] = value.astype(BF16)
                    rs_copy(ch, s, sub, jnp.minimum(d, 2)).start()

        def turn_some(s):
            @pl.when(main)
            def _():
                lax.fori_loop(4 * s, jnp.minimum(4 * s + 4, turns), turn_up, 0)

        tc = 512

        def all_terms(b, carry):
            sl = pl.ds(pl.multiple_of(b * tc, tc), tc)
            terms[sl, :] = jnp.dot(dnt[sl, :], ht[...], preferred_element_type=F32)
            return carry

        steps = half // 2
        step(0, (3,), (0, 1, 2))
        lax.fori_loop(0, terms.shape[0] // tc, all_terms, 0)
        turn_some(0)
        step(1, (), (3,))
        turn_some(1)

        def steady(s, carry):
            step(s, (), ())

            turn_some(s)
            return carry

        lax.fori_loop(2, steps, steady, 0)
        @pl.when(main)
        def _():
            up_copy.start()
            own_up.start()

        for sub in range(2):
            total = terms[rows_of(z, sub), :]
            for ch in range(4):
                rs_copy(ch, steps - 1, sub, 2).wait_recv()
                total = total + rs_in[ch, steps - 1, sub].astype(F32)
            outb[pl.ds(sub * rows, rows), :] = total.astype(BF16)
        out_copy.start()
        own_out.start()

        def rs_sent(s, carry):
            for sub in range(2):
                for ch in range(3):
                    rs_copy(ch, s, sub, 2).wait_send()

                @pl.when(s > 0)
                def _():
                    rs_copy(3, s, sub, 2).wait_send()

            return carry

        lax.fori_loop(0, steps, rs_sent, 0)
        out_copy.wait_send()
        own_out.wait()

    @pl.when(main)
    def _():
        for k in range(pieces):
            rows_copy(k).wait_send()
        down_copy(left, 0, 0, 1).wait_send()
        down_copy(right, 1, 1, 1).wait_send()
        for d in range(2):
            for k in range(2):
                down_copy(x, k, d, 0).wait_send()
        for k, xs in enumerate((x, left, right, far)):
            down_across(xs, k, True).wait_send()

        def sent(i, carry):
            y_copy(i, True).wait_send()
            for k in range(2):
                x_copy(x, k, i, k * per_col + i, True).wait_send()
                x_copy(x, k, i, k * per_col + i, False).wait_send()

                @pl.when(i % 2 == 0)
                def _():
                    x_copy(left, k, i, relay_slot(k, i), True).wait_send()

                @pl.when(i % 2 == 1)
                def _():
                    x_copy(right, k, i, relay_slot(k, i), False).wait_send()

            return carry

        lax.fori_loop(0, per_col, sent, 0)
        dn_copy.wait_send()
        up_copy.wait_send()
        own_dn = pltpu.make_async_copy(half_of(dn, par, hid), dn_ref, l_sem.at[0])
        own_dn.wait()
        own_up.wait()

    @pl.when(apart)
    def _():
        dnt_copy.wait_send()
        ht_copy.wait_send()

    @pl.when(agent)
    def _():
        loads[3].wait()
        dn_copy.wait_recv()
        up_copy.wait_recv()

    @pl.when(c == 0)
    def _():
        out_copy.wait_recv()

    @pl.when(agent)
    def _():
        def scattered(j, carry):
            scatter_copy(j).wait_send()
            return carry

        lax.fori_loop(0, per_col, scattered, 0)


def result_kernel(*refs):
    sources, results, buffers, (in_sem, out_sem) = refs[:3], refs[3:6], refs[6:9], refs[9:]
    reads, writes = [], []
    for k in range(3):
        size = sources[k].shape[0] // 2 // 16 * 16
        for part, sl in enumerate((pl.ds(0, size), pl.ds(size, sources[k].shape[0] - size))):
            reads.append(pltpu.make_async_copy(sources[k].at[sl], buffers[k].at[sl], in_sem.at[k, part]))
            writes.append(pltpu.make_async_copy(buffers[k].at[sl], results[k].at[sl], out_sem.at[k, part]))
    for read in reads:
        read.start()
    for read, write in zip(reads, writes):
        read.wait()
        write.start()
    for write in writes:
        write.wait()


def solution(mesh):
    nz, nx = mesh.shape["fs"] // 2, mesh.shape["tp"]

    def shards(tokens, up_master, down_master, norm_gain):
        rows = up_master.shape[0]
        hid, dcols = down_master.shape
        count, width = tokens.shape
        feat, wide = 2 * rows, 2 * hid
        steps = nz // 4
        per_col = nz // nx
        dma = pltpu.SemaphoreType.DMA
        any_space = pl.BlockSpec(memory_space=pltpu.HBM)
        results = pl.pallas_call(
            functools.partial(kernel, nz, nx),
            out_shape=(
                jax.ShapeDtypeStruct((rows, count), BF16),
                jax.ShapeDtypeStruct((hid, width), BF16),
                jax.ShapeDtypeStruct((hid, width), BF16),
            ),
            in_specs=[any_space] * 4,
            out_specs=(any_space,) * 3,
            scratch_shapes=[
                pltpu.VMEM((count, width), BF16),
                pltpu.VMEM(up_master.shape, F32),
                pltpu.VMEM(down_master.shape, F32),
                pltpu.VMEM((1, rows), F32),
                pltpu.VMEM(up_master.shape, BF16),
                pltpu.VMEM(up_master.shape, BF16),
                pltpu.VMEM((width, wide), BF16),
                pltpu.VMEM((wide, width), BF16),
                pltpu.VMEM((count, width), BF16),
                pltpu.VMEM((width, wide), BF16),
                pltpu.VMEM((wide, width), BF16),
                pltpu.VMEM((count, wide), F32),
                pltpu.VMEM((wide, count), BF16),
                pltpu.VMEM((width, count), F32),
                pltpu.VMEM((4, steps, 2, rows, count), BF16),
                pltpu.VMEM((4, steps, 2, rows, count), BF16),
                pltpu.VMEM((feat, count), BF16),
                dma((4,)),
                dma((4,)),
                dma((4,)),
                dma((4,)),
                dma((4,)),
                dma((per_col,)),
                dma((per_col,)),
                dma((per_col,)),
                dma((per_col,)),
                dma((2, 3 * per_col)),
                dma((2, 3 * per_col)),
                dma((2, 2, 2)),
                dma((2, 2, 2)),
                dma((4, steps, 2)),
                dma((4, steps, 2)),
                dma((5,)),
                dma((5,)),
                dma((3,)),
            ],
            compiler_params=pltpu.CompilerParams(
                collective_id=0, has_side_effects=True, vmem_limit_bytes=60 * 1024 * 1024
            ),
        )(tokens, up_master, down_master, norm_gain[None])
        out_t, up_t, down = pl.pallas_call(
            result_kernel,
            out_shape=tuple(jax.ShapeDtypeStruct(r.shape, r.dtype) for r in results),
            in_specs=[any_space] * 3,
            out_specs=(any_space,) * 3,
            scratch_shapes=[pltpu.VMEM(r.shape, r.dtype) for r in results] + [dma((3, 2)), dma((3, 2))],
            compiler_params=pltpu.CompilerParams(vmem_limit_bytes=60 * 1024 * 1024),
        )(*results)
        return out_t.T, up_t.T, down

    return jax.shard_map(
        shards,
        mesh=mesh,
        in_specs=(P(("grp", "tp"), None), P("fs", "tp"), P("fs", "tp"), P("fs")),
        out_specs=(P(("grp", "tp"), "fs"), P("grp", "fs"), P(("grp", "fs"), None)),
        check_vma=False,
    )
```

```python
import functools

import jax
import jax.numpy as jnp
from jax import lax
from jax.experimental import pallas as pl
from jax.experimental.pallas import tpu as pltpu
from jax.sharding import PartitionSpec as P

MESH = pl.DeviceIdType.MESH
BF16 = jnp.bfloat16
F32 = jnp.float32


def kernel(
    nz, nx, tok_hbm, upm_hbm, dnm_hbm, gain_hbm, out_ref, upt_ref, dn_ref,
    tok, upm, dnm, gain, stage, slots, up, dn, nrm, dnt, upt, acc, ht, terms, rs_out, rs_in, outb,
    in_sem, xa_send, xa_recv, dy_send, dy_recv, zs_send, zs_recv, y_send, y_recv, x_send, x_recv, dn_send, dn_recv,
    rs_send, rs_recv, o_send, o_recv, l_sem,
):
    g, fs, x = lax.axis_index("grp"), lax.axis_index("fs"), lax.axis_index("tp")
    z, c = fs // 2, fs % 2
    par = g % 2
    other = g + 1 - 2 * par
    main = c == par
    agent = c != par
    adds = c == 1
    apart = jnp.logical_and(main, c == 0)
    right, left = (x + 1) % nx, (x + nx - 1) % nx
    per_col = nz // nx
    quarter = z // per_col
    shift = (nx - 1) - z % nx
    served = (x + nx - shift) % nx
    residue = (2 * nx - 1 - x + quarter) % nx
    far = (x + 2) % nx
    half = nz // 2
    rows = upm.shape[0]
    hid = dnm.shape[0]
    dcols = dnm.shape[1]
    wide = 2 * hid
    feat = 2 * rows

    def dev(g_, z_, c_, x_):
        return {"grp": g_, "fs": 2 * z_ + c_, "tp": x_}

    def remote(src, dst, ssem, rsem, to):
        return pltpu.make_async_remote_copy(
            src_ref=src, dst_ref=dst, send_sem=ssem, recv_sem=rsem, device_id=to, device_id_type=MESH
        )

    def up_rows(zs, cs):
        return up.at[pl.ds(pl.multiple_of((2 * zs + cs) * rows, 16), rows), :]

    def dn_part(h, xs):
        return dn.at[pl.ds(h * hid, hid), pl.ds(pl.multiple_of(xs * dcols, 128), dcols)]

    loads = [
        pltpu.make_async_copy(upm_hbm, upm, in_sem.at[0]),
        pltpu.make_async_copy(gain_hbm, gain, in_sem.at[1]),
        pltpu.make_async_copy(dnm_hbm, dnm, in_sem.at[2]),
        pltpu.make_async_copy(tok_hbm, tok, in_sem.at[3]),
    ]
    for k in range(4):
        loads[k].start()

    barrier = pltpu.get_barrier_semaphore()

    def greet(to):
        pl.semaphore_signal(barrier, inc=1, device_id=to, device_id_type=MESH)

    @pl.when(main)
    def _():
        def greet_agent(i, carry):
            greet(dev(g, i * nx + residue, 1 - par, x))
            return carry

        lax.fori_loop(0, per_col, greet_agent, 0)
        for to_x in (right, left):
            greet(dev(g, z, par, to_x))
            greet(dev(other, z, 1 - par, to_x))
        greet(dev(g, z, 1 - par, x))
        greet(dev(other, z, 1 - par, x))

    @pl.when(agent)
    def _():
        greet(dev(g, z, par, x))
        greet(dev(g, z, par, served))

    @pl.when(adds)
    def _():
        for d in (1, 2, nz - 1, nz - 2):
            greet(dev(g, (z + d) % nz, 1, x))

    loads[0].wait()
    loads[1].wait()

    @pl.when(main)
    def _():
        eye = lax.broadcasted_iota(jnp.int32, (rows, rows), 0) == lax.broadcasted_iota(jnp.int32, (rows, rows), 1)
        scale = jnp.sum(jnp.where(eye, gain[...], 0.0), axis=1, keepdims=True)
        stage[...] = (scale * upm[...]).astype(BF16)

    loads[2].wait()

    @pl.when(main)
    def _():
        dn_part(par, x)[...] = dnm[...].astype(BF16)

    peers = jnp.where(main, 7, 1 + per_col) + jnp.where(adds, 4, 0)
    pl.semaphore_wait(barrier, peers)

    pieces = 4
    per_piece = per_col // pieces

    def rows_copy(k):
        sl = pl.ds(k * per_piece * wide, per_piece * wide)
        return remote(
            stage.at[:, sl], slots.at[:, sl], xa_send.at[k], xa_recv.at[k], dev(g, z, 1 - par, (x + shift) % nx)
        )

    @pl.when(main)
    def _():
        for k in range(pieces):
            rows_copy(k).start()

    def scatter_copy(j):
        part = slots.at[:, pl.ds(pl.multiple_of(j * wide, 128), wide)]
        return remote(
            part, up_rows(z, par), zs_send.at[j], zs_recv.at[z // nx], dev(g, per_col * served + j, par, x)
        )

    @pl.when(agent)
    def _():
        for k in range(pieces):
            rows_copy(k).wait_recv()
            for j in range(per_piece):
                scatter_copy(k * per_piece + j).start()

    def to_mate(src, dst, k):
        return remote(src, dst, o_send.at[k], o_recv.at[k], dev(g, z, 1 - c, x))

    def half_of(ref, core, size):
        return ref.at[pl.ds(pl.multiple_of(core * size, 16), size), :]

    up_copy = to_mate(half_of(upt, 1 - par, hid), upt_ref, 0)
    dn_copy = to_mate(half_of(dn, 1 - par, hid), dn_ref, 1)
    out_copy = to_mate(outb.at[pl.ds(0, rows), :], out_ref, 2)
    dnt_copy = to_mate(dnt, dnt, 3)
    ht_copy = to_mate(ht, ht, 4)

    part_rows = hid // 2

    def down_part(xs, k):
        first = pl.multiple_of(par * hid + k * part_rows, 16)
        return dn.at[pl.ds(first, part_rows), pl.ds(pl.multiple_of(xs * dcols, 128), dcols)]

    def down_copy(xs, k, d, relayed):
        part = down_part(xs, k)
        return remote(
            part, part, dn_send.at[d, k, relayed], dn_recv.at[d, k, relayed], dev(g, z, par, left if d else right)
        )

    def down_across(xs, k, mine):
        part = dn_part(par if mine else 1 - par, xs)
        return remote(part, part, dy_send.at[k], dy_recv.at[k], dev(other, z, 1 - par, x))

    def piece(xs, k, i):
        cs = par if k == 0 else 1 - par
        return up_rows(nx * i + (2 * nx - 1 - xs + quarter) % nx, cs)

    def x_copy(xs, k, i, slot, to_right):
        d = 0 if to_right else 1
        part = piece(xs, k, i)
        return remote(part, part, x_send.at[d, slot], x_recv.at[d, slot], dev(g, z, par, right if to_right else left))

    def diagonal(i, to_right):
        d = 0 if to_right else 1
        part, slot = piece(x, 0, i), per_col + i
        return remote(part, part, x_send.at[d, slot], x_recv.at[d, slot], dev(other, z, 1 - par, right if to_right else left))

    def y_copy(i, mine):
        part = piece(x, 0 if mine else 1, i)
        return remote(part, part, y_send.at[i], y_recv.at[i], dev(other, z, 1 - par, x))

    def relay_slot(k, i):
        return 2 * per_col + k * (per_col // 2) + i // 2

    def relay(k, i):

        @pl.when(i % 2 == 0)
        def _():
            x_copy(left, k, i, k * per_col + i, True).wait_recv()
            x_copy(left, k, i, relay_slot(k, i), True).start()

        @pl.when(i % 2 == 1)
        def _():
            x_copy(right, k, i, k * per_col + i, False).wait_recv()
            x_copy(right, k, i, relay_slot(k, i), False).start()

    @pl.when(main)
    def _():
        for k in range(2):
            down_copy(x, k, 0, 0).start()
            down_copy(x, 1 - k, 1, 0).start()
        down_across(x, 0, True).start()

        loads[3].wait()
        block = 64

        def norm(b, carry):
            sl = pl.ds(pl.multiple_of(b * block, block), block)
            values = tok[sl, :].astype(F32)
            center = jnp.mean(values, axis=-1, keepdims=True)
            spread = jnp.mean(jnp.square(values - center), axis=-1, keepdims=True)
            nrm[sl, :] = ((values - center) * lax.rsqrt(spread + 1e-05)).astype(BF16)
            return carry

        lax.fori_loop(0, tok.shape[0] // block, norm, 0)

        down_copy(left, 0, 0, 0).wait_recv()
        down_copy(left, 0, 0, 1).start()
        down_copy(right, 1, 1, 0).wait_recv()
        down_copy(right, 1, 1, 1).start()
        down_copy(left, 1, 0, 0).wait_recv()
        down_across(left, 1, True).start()
        down_copy(right, 0, 1, 0).wait_recv()
        down_across(right, 2, True).start()

        def turn_down(j, carry):
            sl = pl.ds(pl.multiple_of(j * 128, 128), 128)
            dnt[sl, :] = dn[:, sl].T
            return carry

        own_dn = pltpu.make_async_copy(half_of(dn, par, hid), dn_ref, l_sem.at[0])

        def ordered(s):
            away = (s + 1) // 2
            near_first = (z // nx + per_col + jnp.where(s % 2 == 1, away, -away)) % per_col
            falling = (2 * per_col - 2 - s) % per_col
            return jnp.where(quarter < nx // 2, (s + 1) % per_col, jnp.where(quarter < nx - 1, falling, near_first))

        chunk = nx * feat
        acc[...] = jnp.zeros_like(acc)

        def at_lag(s, lag, run):
            @pl.when(jnp.logical_and(s >= lag, s < per_col + lag))
            def _():
                run(ordered(s - lag))

        def arrived(i):
            remote(piece(x, 0, i), piece(x, 0, i), y_send.at[0], zs_recv.at[i], dev(other, z, 1 - par, x)).wait_recv()
            y_copy(i, True).start()
            x_copy(x, 0, i, i, True).start()
            x_copy(x, 0, i, i, False).start()
            diagonal(i, True).start()
            diagonal(i, False).start()

        def crossed(i):
            y_copy(i, False).wait_recv()

        def complete(i):
            for k in range(2):

                @pl.when(i % 2 == 1)
                def _():
                    x_copy(left, k, i, k * per_col + i, True).wait_recv()
                    x_copy(far, k, i, relay_slot(k, i), False).wait_recv()

                @pl.when(i % 2 == 0)
                def _():
                    x_copy(right, k, i, k * per_col + i, False).wait_recv()
                    x_copy(far, k, i, relay_slot(k, i), True).wait_recv()

            sl = pl.ds(pl.multiple_of(i * chunk, 128), chunk)
            acc[...] += jnp.dot(nrm[:, sl], up[sl, :], preferred_element_type=F32)

        def gather_up(s, carry):
            @pl.when(s == 1)
            def _():
                down_copy(far, 0, 0, 1).wait_recv()
                down_copy(far, 1, 1, 1).wait_recv()
                down_across(far, 3, True).start()

            @pl.when(s == 5)
            def _():
                for k, xs in enumerate((x, left, right, far)):
                    down_across(xs, k, False).wait_recv()
                own_dn.start()
                dn_copy.start()
                lax.fori_loop(0, dn.shape[1] // 128, turn_down, 0)

                @pl.when(apart)
                def _():
                    dnt_copy.start()

            at_lag(s, 0, arrived)
            at_lag(s, 2, crossed)
            at_lag(s, 3, lambda i: relay(0, i))
            at_lag(s, 3, lambda i: relay(1, i))
            at_lag(s, 6, complete)
            return carry

        lax.fori_loop(0, per_col + 6, gather_up, 0)

        ht[...] = jnp.square(jnp.maximum(acc[...], 0.0)).T.astype(BF16)

        @pl.when(apart)
        def _():
            ht_copy.start()

    def turn_up(j, carry):
        sl = pl.ds(pl.multiple_of(j * 128, 128), 128)
        upt[:, sl] = up[sl, :].T
        return carry

    turns = up.shape[0] // 128
    own_up = pltpu.make_async_copy(half_of(upt, par, hid), upt_ref, l_sem.at[1])
    own_out = pltpu.make_async_copy(outb.at[pl.ds(rows, rows), :], out_ref, l_sem.at[2])

    @pl.when(apart)
    def _():
        lax.fori_loop(0, turns, turn_up, 0)
        up_copy.start()
        own_up.start()

    @pl.when(jnp.logical_and(agent, adds))
    def _():
        dnt_copy.wait_recv()
        ht_copy.wait_recv()

    @pl.when(adds)
    def _():
        chains = ((1, 0), (1, 1), (-1, 1), (-1, 0))

        def rs_copy(ch, s, sub, dist):
            sign = chains[ch][0]
            to = (z + nz + sign * dist) % nz
            return remote(
                rs_out.at[ch, s, sub], rs_in.at[ch, s, sub], rs_send.at[ch, s, sub], rs_recv.at[ch, s, sub], dev(g, to, 1, x)
            )

        def rows_of(zt, sub):
            return pl.ds(pl.multiple_of(zt * feat + sub * rows, 16), rows)

        def step(s, skip, first_of):
            for sub in range(2):
                for ch in (1, 2, 0, 3):
                    if ch in skip:
                        continue
                    sign, odd = chains[ch]
                    d = half - odd - 2 * s
                    sl = rows_of((z + 2 * nz + sign * d) % nz, sub)
                    if isinstance(s, int) and s == 0:
                        value = jnp.dot(dnt[sl, :], ht[...], preferred_element_type=F32)
                    else:
                        value = terms[sl, :]
                    if ch not in first_of:
                        rs_copy(ch, s - 1, sub, 2).wait_recv()
                        value = value + rs_in[ch, s - 1, sub].astype(F32)
                    rs_out[ch, s, sub] = value.astype(BF16)
                    rs_copy(ch, s, sub, jnp.minimum(d, 2)).start()

        def turn_some(s):
            @pl.when(main)
            def _():
                lax.fori_loop(4 * s, jnp.minimum(4 * s + 4, turns), turn_up, 0)

        tc = 512

        def all_terms(b, carry):
            sl = pl.ds(pl.multiple_of(b * tc, tc), tc)
            terms[sl, :] = jnp.dot(dnt[sl, :], ht[...], preferred_element_type=F32)
            return carry

        steps = half // 2
        step(0, (3,), (0, 1, 2))
        lax.fori_loop(0, terms.shape[0] // tc, all_terms, 0)
        turn_some(0)
        step(1, (), (3,))
        turn_some(1)

        def steady(s, carry):
            step(s, (), ())

            turn_some(s)
            return carry

        lax.fori_loop(2, steps, steady, 0)
        @pl.when(main)
        def _():
            up_copy.start()
            own_up.start()

        for sub in range(2):
            total = terms[rows_of(z, sub), :]
            for ch in range(4):
                rs_copy(ch, steps - 1, sub, 2).wait_recv()
                total = total + rs_in[ch, steps - 1, sub].astype(F32)
            outb[pl.ds(sub * rows, rows), :] = total.astype(BF16)
        out_copy.start()
        own_out.start()

        def rs_sent(s, carry):
            for sub in range(2):
                for ch in range(3):
                    rs_copy(ch, s, sub, 2).wait_send()

                @pl.when(s > 0)
                def _():
                    rs_copy(3, s, sub, 2).wait_send()

            return carry

        lax.fori_loop(0, steps, rs_sent, 0)
        out_copy.wait_send()
        own_out.wait()

    @pl.when(main)
    def _():
        for k in range(pieces):
            rows_copy(k).wait_send()
        down_copy(left, 0, 0, 1).wait_send()
        down_copy(right, 1, 1, 1).wait_send()
        for d in range(2):
            for k in range(2):
                down_copy(x, k, d, 0).wait_send()
        for k, xs in enumerate((x, left, right, far)):
            down_across(xs, k, True).wait_send()

        def sent(i, carry):
            y_copy(i, True).wait_send()
            for k in range(2):
                x_copy(x, k, i, k * per_col + i, True).wait_send()
                x_copy(x, k, i, k * per_col + i, False).wait_send()

                @pl.when(i % 2 == 0)
                def _():
                    x_copy(left, k, i, relay_slot(k, i), True).wait_send()

                @pl.when(i % 2 == 1)
                def _():
                    x_copy(right, k, i, relay_slot(k, i), False).wait_send()

            return carry

        lax.fori_loop(0, per_col, sent, 0)
        dn_copy.wait_send()
        up_copy.wait_send()
        own_dn = pltpu.make_async_copy(half_of(dn, par, hid), dn_ref, l_sem.at[0])
        own_dn.wait()
        own_up.wait()

    @pl.when(apart)
    def _():
        dnt_copy.wait_send()
        ht_copy.wait_send()

    @pl.when(agent)
    def _():
        loads[3].wait()
        dn_copy.wait_recv()
        up_copy.wait_recv()

    @pl.when(c == 0)
    def _():
        out_copy.wait_recv()

    @pl.when(agent)
    def _():
        def scattered(j, carry):
            scatter_copy(j).wait_send()
            return carry

        lax.fori_loop(0, per_col, scattered, 0)


def result_kernel(*refs):
    sources, results, buffers, (in_sem, out_sem) = refs[:3], refs[3:6], refs[6:9], refs[9:]
    reads, writes = [], []
    for k in range(3):
        size = sources[k].shape[0] // 2 // 16 * 16
        for part, sl in enumerate((pl.ds(0, size), pl.ds(size, sources[k].shape[0] - size))):
            reads.append(pltpu.make_async_copy(sources[k].at[sl], buffers[k].at[sl], in_sem.at[k, part]))
            writes.append(pltpu.make_async_copy(buffers[k].at[sl], results[k].at[sl], out_sem.at[k, part]))
    for read in reads:
        read.start()
    for read, write in zip(reads, writes):
        read.wait()
        write.start()
    for write in writes:
        write.wait()


def solution(mesh):
    nz, nx = mesh.shape["fs"] // 2, mesh.shape["tp"]

    def shards(tokens, up_master, down_master, norm_gain):
        rows = up_master.shape[0]
        hid, dcols = down_master.shape
        count, width = tokens.shape
        feat, wide = 2 * rows, 2 * hid
        steps = nz // 4
        per_col = nz // nx
        dma = pltpu.SemaphoreType.DMA
        any_space = pl.BlockSpec(memory_space=pltpu.HBM)
        results = pl.pallas_call(
            functools.partial(kernel, nz, nx),
            out_shape=(
                jax.ShapeDtypeStruct((rows, count), BF16),
                jax.ShapeDtypeStruct((hid, width), BF16),
                jax.ShapeDtypeStruct((hid, width), BF16),
            ),
            in_specs=[any_space] * 4,
            out_specs=(any_space,) * 3,
            scratch_shapes=[
                pltpu.VMEM((count, width), BF16),
                pltpu.VMEM(up_master.shape, F32),
                pltpu.VMEM(down_master.shape, F32),
                pltpu.VMEM((1, rows), F32),
                pltpu.VMEM(up_master.shape, BF16),
                pltpu.VMEM(up_master.shape, BF16),
                pltpu.VMEM((width, wide), BF16),
                pltpu.VMEM((wide, width), BF16),
                pltpu.VMEM((count, width), BF16),
                pltpu.VMEM((width, wide), BF16),
                pltpu.VMEM((wide, width), BF16),
                pltpu.VMEM((count, wide), F32),
                pltpu.VMEM((wide, count), BF16),
                pltpu.VMEM((width, count), F32),
                pltpu.VMEM((4, steps, 2, rows, count), BF16),
                pltpu.VMEM((4, steps, 2, rows, count), BF16),
                pltpu.VMEM((feat, count), BF16),
                dma((4,)),
                dma((4,)),
                dma((4,)),
                dma((4,)),
                dma((4,)),
                dma((per_col,)),
                dma((per_col,)),
                dma((per_col,)),
                dma((per_col,)),
                dma((2, 3 * per_col)),
                dma((2, 3 * per_col)),
                dma((2, 2, 2)),
                dma((2, 2, 2)),
                dma((4, steps, 2)),
                dma((4, steps, 2)),
                dma((5,)),
                dma((5,)),
                dma((3,)),
            ],
            compiler_params=pltpu.CompilerParams(
                collective_id=0, has_side_effects=True, vmem_limit_bytes=60 * 1024 * 1024
            ),
        )(tokens, up_master, down_master, norm_gain[None])
        out_t, up_t, down = pl.pallas_call(
            result_kernel,
            out_shape=tuple(jax.ShapeDtypeStruct(r.shape, r.dtype) for r in results),
            in_specs=[any_space] * 3,
            out_specs=(any_space,) * 3,
            scratch_shapes=[pltpu.VMEM(r.shape, r.dtype) for r in results] + [dma((3, 2)), dma((3, 2))],
            compiler_params=pltpu.CompilerParams(vmem_limit_bytes=60 * 1024 * 1024),
        )(*results)
        return out_t.T, up_t.T, down

    return jax.shard_map(
        shards,
        mesh=mesh,
        in_specs=(P(("grp", "tp"), None), P("fs", "tp"), P("fs", "tp"), P("fs")),
        out_specs=(P(("grp", "tp"), "fs"), P("grp", "fs"), P(("grp", "fs"), None)),
        check_vma=False,
    )
```
